32 devices in a mesh: sp: 4 (over y, x), tp: 8 (over z, core).
Axes of the slice: x: 2, y: 2, z: 4, core: 2. Of those that a mesh axis runs over, the one named last changes fastest.
Arguments:
- gate_b: bfloat16 [2048, 1024], P('sp', 'tp'), may hold values from -6 to 6
- gate_c: bfloat16 [2048, 1024], P('sp', 'tp'), may hold values from -6 to 6
- values_in: bfloat16 [2048, 1024], P('sp', 'tp'), may hold values from -6 to 6
- conv_w: bfloat16 [3, 1024], P(None, 'tp'), may hold values from -3.5 to 3.5
- documents: int32 [2048], P('sp'), may hold values from 0 to 2, never falling along the last dimension, each value on 1 to 1024 neighbouring positions
- w_out: bfloat16 [1024, 2048], replicated, may hold values from -0.1875 to 0.1875
- resid: bfloat16 [2048, 2048], P(('sp', 'tp')), may hold values from -6 to 6
- norm_gain: bfloat16 [2048], replicated, may hold values from 0.099609375 to 1.8984375
- route_ids: int32 [2048, 2], P(('sp', 'tp')), may hold values from 0 to 3, all different within a row; in each aligned block of 64 rows (0 to 63, 64 to 127, ...) at most 64 rows name the same one
- route_weight: float32 [2048, 2], P(('sp', 'tp')), may hold values from 0.2 to 1
- w_gate: bfloat16 [4, 2048, 7168], P('sp', None, 'tp'), may hold values from -0.125 to 0.125
- w_up: bfloat16 [4, 2048, 7168], P('sp', None, 'tp'), may hold values from -0.125 to 0.125
- w_down: bfloat16 [4, 7168, 2048], P('sp', 'tp'), may hold values from -0.0625 to 0.0625
Outputs:
- layer_out: bfloat16 [2048, 2048], P(('sp', 'tp'))
The draws below stay inside these ranges and needn't reach their ends.
Inputs may be any that keep to these rules, and one draw needn't show every extreme that they name: `route_ids`: each token names two different experts; in the rows of one device no expert is named by more than 64 rows, a bound that some block reaches. `documents`: document numbers never fall along the positions; a document has at most 2048 // 2 positions.
All inputs are finite; a program needn't handle non-finite values.
Results may differ from the reference program's by a relative error of at most 0.018.
Values may be sent and summed in bfloat16 or wider, within the bound.
A program may use at most 128 MiB of HBM per device.

```python
import math
import jax
import jax.numpy as jnp
import numpy as np
from jax import lax

D = 2048
CH = 1024
FF_E = 7168
KW = 3
TOKENS = 2048
ROWS = 64
EXPERTS = 4
CAP = 64
N_SP = 4
N_TP = 8


def shard_levels(key, extent, cuts, least, high):
    gain, own = 1.0, jax.random.fold_in(key, 6)
    for dim, shards_of in cuts:
        draws = jnp.exp(jax.random.uniform(jax.random.fold_in(own, dim), (shards_of,), jnp.float32, least / len(cuts), high / len(cuts)))
        gain = gain * jnp.repeat(draws, extent[dim] // shards_of).reshape([-1 if axis == dim else 1 for axis in range(len(extent))])
    return gain


def profile(number_of, total, bound, skew):
    portions = [(1 << 20) // math.isqrt(rank ** skew) + 1 for rank in range(2, number_of + 1)]
    surplus, counts = total - bound - (number_of - 1), [1] * (number_of - 1)
    while surplus > 0:
        candidates = [i for i in range(number_of - 1) if counts[i] < bound]
        mass, left = sum([portions[i] for i in candidates]), surplus
        for i in candidates:
            addition = min(bound - counts[i], max(1, left * portions[i] // mass), surplus)
            counts[i] = counts[i] + addition
            surplus = surplus - addition
    return np.array([bound] + counts)


def ragged_sizes(stream_key, amount, total, limit, skew):
    if amount == 2:
        one = jax.random.randint(stream_key, (), max(1, total - limit), min(limit, total - 1) + 1)
        return jnp.stack([one, total - one])
    lengths = jnp.asarray(profile(amount, total, limit, skew), jnp.int32)
    couples = (amount - 1) // 2
    giver, sink = lengths[1:1 + 2 * couples:2], lengths[2:2 + 2 * couples:2]
    slack = jnp.minimum(giver - 1, limit - sink)
    moved = jax.random.randint(jax.random.fold_in(stream_key, 1), (couples,), 0, 1 << 20) % (slack + 1)
    lengths = lengths.at[1:1 + 2 * couples:2].set(giver - moved).at[2:2 + 2 * couples:2].set(sink + moved)
    return lengths[jax.random.permutation(jax.random.fold_in(stream_key, 2), amount)]


def assign_block(own_key, own, number, rows, number_of, top, limit, skew):
    order = jax.random.permutation(own_key, number_of)
    crowded, common = shares(number_of, rows * top, limit, skew, True), shares(number_of, rows * top, limit, skew, False)
    places = jnp.arange(number_of)

    def named(lengths, rotation):
        used = int((lengths > 0).sum())
        fixed = max(1, used // 4)
        shifted = fixed + (places - fixed + rotation * (used - fixed)) % max(1, number_of - fixed)
        return jnp.zeros((number_of,), jnp.int32).at[order[jnp.where(places < fixed, places, shifted)]].set(jnp.asarray(lengths, jnp.int32))

    lengths = jnp.where(number % 4 == 0, named(crowded, number // 4), named(common, number - number // 4 - 1))
    mixed = jax.random.permutation(jax.random.fold_in(own, 3), number_of)
    giver, receiver = mixed[0:number_of // 2 * 2:2], mixed[1:number_of // 2 * 2:2]
    slack = jnp.minimum(lengths[giver] - 1, limit - lengths[receiver]) // 2
    slack = jnp.where((giver == order[0]) | (receiver == order[0]) | (lengths[receiver] == 0), 0, jnp.maximum(slack, 0))
    shifted = jax.random.randint(jax.random.fold_in(own, 4), (number_of // 2,), 0, 1 << 20) % (slack + 1)
    lengths = lengths.at[giver].add(-shifted).at[receiver].add(shifted)
    items = jnp.searchsorted(jnp.cumsum(lengths), jnp.arange(rows * top), side="right").astype(jnp.int32)
    listing = items.reshape(top, rows).T
    listing = listing[jax.random.permutation(jax.random.fold_in(own, 1), rows)]
    rotation = jax.random.randint(jax.random.fold_in(own, 2), (rows, 1), 0, top)
    return jnp.take_along_axis(listing, (jnp.arange(top)[None, :] + rotation) % top, axis=1)


def shares(count, total, bound, lean, full):
    loads = [(1 << 20) // math.isqrt(grade ** lean) + 1 for grade in range(1, count + 1)]
    largest = bound if full else min(bound, max(-(-total // count), total * loads[0] // sum(loads)))
    least = 1 if total - largest >= count - 1 else 0
    counts, spare = [largest] + [least] * (count - 1), total - largest - least * (count - 1)
    while spare > 0:
        movable = [i for i in range(1, count) if counts[i] < largest] or [i for i in range(1, count) if counts[i] < bound]
        mass, remaining = sum([loads[i] for i in movable]), spare
        for i in movable:
            addition = min(bound - counts[i], max(1, remaining * loads[i] // mass), spare)
            counts[i] = counts[i] + addition
            spare = spare - addition
    return np.array(counts)


def centred(stream_key, dims, deviation, most, cuts=(), held_as=jnp.bfloat16):
    factor_of = shard_levels(stream_key, dims, cuts, -0.22, 0.18) if cuts else 1.0
    result = jax.random.normal(stream_key, dims, jnp.float32) * deviation * factor_of
    return jnp.minimum(jnp.maximum(result, -most), most).astype(held_as)


def setup_inputs(seed: int = 0) -> dict:
    arg_keys = jax.random.split(jax.random.key(seed), 14)
    gate_b = centred(arg_keys[0], (TOKENS, CH), 1.0, 6.0, ((0, 4), (1, 8)))
    gate_c = centred(arg_keys[1], (TOKENS, CH), 1.0, 6.0, ((0, 4), (1, 8)))
    values_in = centred(arg_keys[2], (TOKENS, CH), 1.0, 6.0, ((0, 4), (1, 8)))
    conv_w = centred(arg_keys[3], (KW, CH), KW ** -0.5, 3.5, ((1, 8),))
    documents = jnp.searchsorted(jnp.cumsum(ragged_sizes(arg_keys[4], N_SP // 2 + 1, TOKENS, TOKENS // 2, 1)), jnp.arange(TOKENS), side="right").astype(jnp.int32)
    w_out = centred(arg_keys[5], (CH, D), CH ** -0.5, 0.1875)
    resid = centred(arg_keys[6], (TOKENS, D), 1.0, 6.0, ((0, 32),))
    norm_gain = jnp.clip(1.0 + 0.18 * jax.random.normal(arg_keys[7], (D,), jnp.float32), 0.099609375, 1.8984375).astype(jnp.bfloat16)
    route_ids_keys = jax.random.split(jax.random.fold_in(arg_keys[8], 1), TOKENS // ROWS)
    route_ids_turns = jax.random.permutation(jax.random.fold_in(arg_keys[8], 3), TOKENS // ROWS)
    route_ids = jax.vmap(lambda own, number: assign_block(jax.random.fold_in(arg_keys[8], 2), own, number, ROWS, EXPERTS, 2, CAP, 2))(route_ids_keys, route_ids_turns).reshape((TOKENS, 2))
    route_weight = jnp.clip(0.2 + 0.8 * jax.random.uniform(arg_keys[9], (TOKENS, 2), jnp.float32) ** shard_levels(arg_keys[9], (TOKENS, 2), ((0, 32),), -0.2, 0.2), 0.2, 1.0)
    w_gate = centred(arg_keys[10], (EXPERTS, D, FF_E), D ** -0.5, 0.125, ((0, 4), (2, 8)))
    w_up = centred(arg_keys[11], (EXPERTS, D, FF_E), D ** -0.5, 0.125, ((0, 4), (2, 8)))
    w_down = centred(arg_keys[12], (EXPERTS, FF_E, D), FF_E ** -0.5, 0.0625, ((0, 4), (1, 8)))
    return {"gate_b": gate_b, "gate_c": gate_c, "values_in": values_in, "conv_w": conv_w, "documents": documents, "w_out": w_out, "resid": resid, "norm_gain": norm_gain, "route_ids": route_ids, "route_weight": route_weight, "w_gate": w_gate, "w_up": w_up, "w_down": w_down}


def reference(gate_b, gate_c, values_in, conv_w, documents, w_out, resid, norm_gain, route_ids, route_weight, w_gate, w_up, w_down):
    product = gate_c.astype(jnp.float32) * values_in.astype(jnp.float32)
    padded = jnp.concatenate([jnp.zeros((2, CH), jnp.float32), product], axis=0)
    padded_docs = jnp.concatenate([jnp.full((2,), -1, jnp.int32), documents], axis=0)
    kernel_taps = conv_w.astype(jnp.float32)
    near_mask = (padded_docs[1:-1] == documents).astype(jnp.float32)[:, None]
    far_mask = (padded_docs[:-2] == documents).astype(jnp.float32)[:, None]
    convolved = kernel_taps[2] * product + kernel_taps[1] * padded[1:-1] * near_mask + kernel_taps[0] * padded[:-2] * far_mask
    mixed_rows = (gate_b.astype(jnp.float32) * convolved).astype(jnp.bfloat16)
    projected = jnp.dot(mixed_rows, w_out, preferred_element_type=jnp.float32)
    hidden_state = (resid.astype(jnp.float32) + projected).astype(jnp.bfloat16)
    state_wide = hidden_state.astype(jnp.float32)
    normed = (state_wide * lax.rsqrt(lax.optimization_barrier(jnp.mean(state_wide * state_wide, axis=-1, keepdims=True)) + 1e-06) * norm_gain.astype(jnp.float32)).astype(jnp.bfloat16)
    blocks = TOKENS // ROWS
    block_ids = route_ids.reshape(blocks, 2 * ROWS)
    one_hot = (block_ids[:, :, None] == jnp.arange(EXPERTS, dtype=jnp.int32)[None, None, :]).astype(jnp.int32)
    rank_in = lax.optimization_barrier(jnp.sum((jnp.cumsum(one_hot, axis=1) - one_hot) * one_hot, axis=2))
    per_expert = blocks * CAP
    block_index = jnp.arange(blocks, dtype=jnp.int32)[:, None]
    flat_slot = (block_ids * per_expert + block_index * CAP + rank_in).astype(jnp.int32)
    token_index = (block_index * ROWS + jnp.arange(2 * ROWS, dtype=jnp.int32)[None, :] // 2).astype(jnp.int32)
    slot_table = jnp.full((EXPERTS * per_expert,), TOKENS, jnp.int32).at[flat_slot.reshape(-1)].set(token_index.reshape(-1))
    padded_rows = jnp.concatenate([normed, jnp.zeros((1, D), jnp.bfloat16)], axis=0)

    def serve_expert(operands):
        slot_rows, gate_weight, up_weight, down_weight = operands
        chosen = padded_rows[slot_rows]
        gate_part = jnp.dot(chosen, gate_weight, preferred_element_type=jnp.float32)
        up_part = jnp.dot(chosen, up_weight, preferred_element_type=jnp.float32)
        activated = (jax.nn.silu(gate_part) * up_part).astype(jnp.bfloat16)
        pieces = jnp.einsum('snf,nfd->snd', activated.reshape(per_expert, N_TP, FF_E // N_TP).astype(jnp.float32), down_weight.reshape(N_TP, FF_E // N_TP, D).astype(jnp.float32))
        rounded = lax.optimization_barrier(pieces.astype(jnp.bfloat16))
        return lax.optimization_barrier(jnp.sum(rounded.astype(jnp.float32), axis=1)).astype(jnp.bfloat16)
    expert_out = lax.map(serve_expert, (slot_table.reshape(EXPERTS, per_expert), w_gate, w_up, w_down))
    picked = expert_out.reshape(EXPERTS * per_expert, D)[flat_slot.reshape(TOKENS, 2)]
    combined = lax.optimization_barrier(jnp.sum(route_weight[:, :, None].astype(jnp.float32) * picked.astype(jnp.float32), axis=1))
    return (hidden_state.astype(jnp.float32) + combined).astype(jnp.bfloat16)
```

```python
import functools

import jax
import jax.numpy as jnp
from jax import lax
from jax.experimental import pallas as pl
from jax.experimental.pallas import tpu as pltpu
from jax.sharding import PartitionSpec as P

MESH = pl.DeviceIdType.MESH
LANES = 128


def moe_kernel(
    gb_hbm, gc_hbm, vals_hbm, taps_hbm, docs_hbm, resid_hbm, gain_hbm, ids_hbm, route_hbm,
    wo_hbm, wg_hbm, wu_hbm, wd_hbm, out_ref,
    gb, gc, vals, taps, docs, resid, gain, ids, route,
    hid, tok, mixed, pad, dpad, mat, hc, hv, hd, wo,
    xbuf, pbuf, dbuf, r1, r2, rz, wg, wu, wd,
    in_sem, w_sem,
    s_a, r_a, s_b, s_h, r_h3,
    s_z, r_z, s_1, s_2, r_h, s_p, r_p,
    s_d, r_d, s_r1, r_r1, s_r2, r_r2, s_rz, r_rz,
):
    f32 = jnp.float32
    n_sp, n_tp = lax.axis_size("sp"), lax.axis_size("tp")
    nz = n_tp // 2
    width = out_ref.shape[1]
    half = width // 2
    rows = out_ref.shape[0]
    seq = gb.shape[0]
    halo = hc.shape[0]
    sp, tp = lax.axis_index("sp"), lax.axis_index("tp")
    y, x = sp // 2, sp % 2
    z, c = tp // 2, tp % 2
    xn, yn, dg = y * 2 + 1 - x, (1 - y) * 2 + x, (1 - y) * 2 + 1 - x
    columns = (sp, xn, yn, dg)
    OWN, XN, YN, DG = range(4)
    other = (sp, z * 2 + 1 - c)
    following, previous = (lax.rem(sp + 1, n_sp), tp), (lax.rem(sp + n_sp - 1, n_sp), tp)
    to_x, to_y = (xn, tp), (yn, tp)

    def zz(k):
        if k < 2:
            return 2 * (z // 2) + (z + k) % 2
        return k + (z // 2) * (nz - 1 - 2 * k)

    def slot(k, rel):
        return zz(k) * n_sp + columns[rel]

    def lanes(h):
        return pl.ds(0, half) if h == 0 else pl.ds(half, xbuf.shape[3] - half)

    def cols(h):
        return pl.ds(h * half, half)

    def rc(src, dst, ss, rs, dev):
        return pltpu.make_async_remote_copy(
            src_ref=src, dst_ref=dst, send_sem=ss, recv_sem=rs,
            device_id=dev, device_id_type=MESH,
        )


    def halo_copies():
        pairs = (
            (gc.at[pl.ds(seq - halo, halo)], hc),
            (vals.at[pl.ds(seq - halo, halo)], hv),
            (docs, hd),
        )
        return [rc(a, b, s_h.at[n], r_h3.at[n], following) for n, (a, b) in enumerate(pairs)]

    def channels(j):
        return pl.ds(pl.multiple_of(j * gb.shape[1], gb.shape[1]), gb.shape[1])

    def token_rows(j):
        return mixed.at[pl.ds(pl.multiple_of(j * rows, rows), rows)]

    def swap(d):
        j = lax.rem(tp + d, n_tp)
        return rc(token_rows(j), tok.at[:, channels(tp)], s_a.at[d], r_a.at[tp], (sp, j))

    def swapped(d):
        j = lax.rem(tp + d, n_tp)
        return rc(token_rows(j), tok.at[:, channels(j)], s_a.at[d], r_a.at[j], (sp, j))

    def swap_first():
        return rc(token_rows(0), tok.at[:, channels(tp)], s_b, r_a.at[tp], (sp, 0))

    def convolve(first, count):
        own = pl.ds(first, count)
        now = dpad[pl.ds(first + 8, count)]
        near = (dpad[pl.ds(first + 7, count)] == now).astype(f32)
        far = (dpad[pl.ds(first + 6, count)] == now).astype(f32)
        tap = taps[...].astype(f32)
        convolved = (
            tap[2:3] * pad[pl.ds(first + 8, count)]
            + tap[1:2] * pad[pl.ds(first + 7, count)] * near
            + tap[0:1] * pad[pl.ds(first + 6, count)] * far
        )
        mixed[own] = (gb[own].astype(f32) * convolved).astype(mixed.dtype)

    def mix():
        mat[...] = jnp.zeros_like(mat)
        doc_rows = docs.shape[0]
        mat[pl.ds(0, doc_rows)] = docs[...].astype(f32)
        mat[pl.ds(doc_rows, 2), pl.ds(0, rows)] = ids[...].astype(f32)
        mat[pl.ds(doc_rows + 2, 2), pl.ds(0, rows)] = route[...]
        turned = mat[...].T
        for n in range(doc_rows):
            dpad[pl.ds(8 + n * LANES, LANES)] = jnp.broadcast_to(
                turned[:, n : n + 1], (LANES, dpad.shape[1])
            )
        pad[pl.ds(8, seq)] = gc[...].astype(f32) * vals[...].astype(f32)
        pad[pl.ds(0, 8)] = jnp.zeros((8, pad.shape[1]), f32)
        dpad[pl.ds(0, 8)] = jnp.full((8, dpad.shape[1]), -1.0, f32)
        convolve(0, seq)
        for d in range(1, n_tp):
            @pl.when(lax.rem(tp + d, n_tp) != 0)
            def _():
                swap(d).start()

        lane = lax.broadcasted_iota(jnp.int32, (rows, LANES), 1)
        named = (lane % n_sp).astype(f32)
        part = lane // n_sp
        side = turned[:rows]
        at = doc_rows
        share = jnp.where(side[:, at : at + 1] == named, side[:, at + 2 : at + 3], 0.0) + jnp.where(
            side[:, at + 1 : at + 2] == named, side[:, at + 3 : at + 4], 0.0
        )
        high = share.astype(jnp.bfloat16).astype(f32)
        middle = (share - high).astype(jnp.bfloat16).astype(f32)
        low = share - high - middle
        terms = jnp.where(part == 0, high, jnp.where(part == 1, middle, jnp.where(part == 2, low, 0.0)))
        mine = z * n_sp + sp
        xbuf[c, mine, :, pl.ds(width, LANES)] = terms.astype(xbuf.dtype)

        for copy in halo_copies():
            copy.wait_recv()
        pad[pl.ds(0, 8)] = (hc[...].astype(f32) * hv[...].astype(f32))[halo - 8 :]
        last = hd[pl.ds(doc_rows - 1, 1)].astype(f32)
        last = jnp.where(sp == 0, -1.0, last)
        for n in (1, 2):
            dpad[pl.ds(8 - n, 1)] = jnp.broadcast_to(
                last[:, LANES - n : LANES - n + 1], (1, dpad.shape[1])
            )
        convolve(0, 16)

        @pl.when(tp != 0)
        def _():
            swap_first().start()

        tok[:, channels(tp)] = mixed[pl.ds(pl.multiple_of(tp * rows, rows), rows)]
        in_copies[5].wait()
        in_copies[6].wait()
        wo_copy.wait()
        for d in range(1, n_tp):
            swapped(d).wait_recv()
        projected = jnp.dot(tok[...], wo[...], preferred_element_type=f32)
        hidden = (resid[...].astype(f32) + projected).astype(hid.dtype)
        hid[...] = hidden
        state = hidden.astype(f32)
        scale = lax.rsqrt(jnp.mean(state * state, axis=-1, keepdims=True) + 1e-06)
        for n in range(width // LANES):
            at = slice(n * LANES, (n + 1) * LANES)
            xbuf[c, mine, :, pl.ds(n * LANES, LANES)] = (
                state[:, at] * scale * gain[n : n + 1].astype(f32)
            ).astype(xbuf.dtype)


    def z_send(k):
        at = xbuf.at[c, z * n_sp + sp]
        return rc(at, at, s_z.at[k], r_z.at[z], (sp, zz(k) * 2 + c))

    def z_recv(k):
        at = xbuf.at[c, slot(k, OWN)]
        return rc(at, at, s_z.at[k], r_z.at[zz(k)], (sp, zz(k) * 2 + c))

    def piece(h, rel, k, ss, there, dev):
        at = xbuf.at[c, slot(k, rel), :, lanes(h)]
        return rc(at, at, ss, r_h.at[h, there, k], dev)

    def first(h, k):
        return piece(h, OWN, k, s_1.at[h, k], YN if h == 0 else XN, to_y if h == 0 else to_x)

    def second(h, k):
        return piece(h, OWN, k, s_2.at[h, 0, k], XN if h == 0 else YN, to_x if h == 0 else to_y)

    def third(h, k):
        return piece(h, YN if h == 0 else XN, k, s_2.at[h, 1, k], DG, to_x if h == 0 else to_y)

    def arrived(h, rel, k):
        piece(h, rel, k, s_1.at[h, k], rel, other).wait_recv()

    def to_other(rel, k):
        at = xbuf.at[c, slot(k, rel)]
        return rc(at, at, s_p.at[k * n_sp + rel], r_p.at[k * n_sp + rel], other)

    def spread(k):
        for h in (1, 0):
            first(h, k).start()
        for h in (0, 1):
            second(h, k).start()
        to_other(OWN, k).start()

    def take(k):
        z_recv(k).wait_recv()
        spread(k)

    def relay(k):
        arrived(0, YN, k)
        third(0, k).start()
        arrived(1, XN, k)
        third(1, k).start()

    def sides(k):
        arrived(0, XN, k)
        to_other(XN, k).start()
        arrived(1, YN, k)
        to_other(YN, k).start()

    def corner(k):
        arrived(0, DG, k)
        arrived(1, DG, k)
        to_other(DG, k).start()


    def group(k):
        return pl.ds(zz(k) * n_sp, n_sp)

    def d_copy(k):
        return rc(pbuf.at[1 - c, group(k)], dbuf.at[group(k)], s_d.at[k], r_d.at[k], other)

    def merge(k):
        d_copy(k).wait_recv()
        i = group(k)
        pbuf[c, i] = (pbuf[c, i].astype(f32) + dbuf[i].astype(f32)).astype(pbuf.dtype)

    def r1_copy(h, o, k):
        rel = DG if o else (XN if h == 0 else YN)
        at = pbuf.at[c, slot(k, rel), :, cols(h)]
        return rc(at, r1.at[h, o, k], s_r1.at[h, o, k], r_r1.at[h, o, k], to_x if h == 0 else to_y)

    def r2_copy(h, k):
        at = pbuf.at[c, slot(k, YN if h == 0 else XN), :, cols(h)]
        return rc(at, r2.at[h, k], s_r2.at[h, k], r_r2.at[h, k], to_y if h == 0 else to_x)

    def rz_copy(k):
        at = pbuf.at[c, slot(k, OWN)]
        return rc(at, rz.at[z], s_rz.at[k], r_rz.at[z], (sp, zz(k) * 2 + c))

    def rz_recv(k):
        at = pbuf.at[c, slot(k, OWN)]
        return rc(at, rz.at[zz(k)], s_rz.at[k], r_rz.at[zz(k)], (sp, zz(k) * 2 + c))

    def stage1(k, parts=(1, 0)):
        for o in parts:
            for h in (0, 1):
                r1_copy(h, o, k).start()

    def stage2(k):
        for h in (0, 1):
            r1_copy(h, 1, k).wait_recv()
            i = slot(k, YN if h == 0 else XN)
            pbuf[c, i, :, cols(h)] = (
                pbuf[c, i, :, cols(h)].astype(f32) + r1[h, 1, k].astype(f32)
            ).astype(pbuf.dtype)
            r2_copy(h, k).start()

    def summed(h, k):
        r1_copy(h, 0, k).wait_recv()
        r2_copy(h, k).wait_recv()
        return (
            pbuf[c, slot(k, OWN), :, cols(h)].astype(f32)
            + r1[h, 0, k].astype(f32)
            + r2[h, k].astype(f32)
        )

    def stage3(k):
        for h in (0, 1):
            pbuf[c, slot(k, OWN), :, cols(h)] = summed(h, k).astype(pbuf.dtype)
        rz_copy(k).start()

    barrier = pltpu.get_barrier_semaphore()
    peers = [to_x, to_y, following, previous] + [(sp, lax.rem(tp + d, n_tp)) for d in range(1, n_tp)]
    for peer in peers:
        pl.semaphore_signal(barrier, inc=1, device_id=peer, device_id_type=MESH)
    in_copies = [
        pltpu.make_async_copy(a, b, in_sem.at[n])
        for n, (a, b) in enumerate((
            (gc_hbm, gc), (vals_hbm, vals), (docs_hbm, docs), (taps_hbm, taps), (gb_hbm, gb),
            (resid_hbm, resid), (gain_hbm, gain), (ids_hbm, ids), (route_hbm, route),
        ))
    ]
    weights = [
        pltpu.make_async_copy(a, b, w_sem.at[n])
        for n, (a, b) in enumerate(((wg_hbm, wg), (wu_hbm, wu), (wd_hbm, wd)))
    ]
    wo_copy = pltpu.make_async_copy(wo_hbm, wo, w_sem.at[3])
    for copy in in_copies:
        copy.start()
    wo_copy.start()
    for w in weights:
        w.start()
    for n in (0, 1, 2):
        in_copies[n].wait()
    pl.semaphore_wait(barrier, len(peers))
    for copy in halo_copies():
        copy.start()
    for n in (3, 4, 7, 8):
        in_copies[n].wait()
    mix()
    for h in (1, 0):
        first(h, 0).start()
    for k in range(1, nz):
        z_send(k).start()
    for h in (0, 1):
        second(h, 0).start()
    to_other(OWN, 0).start()
    relay(0)
    take(1)
    sides(0)
    corner(0)
    for w in weights:
        w.wait()

    lane = lax.broadcasted_iota(jnp.int32, (1, LANES), 1)
    chosen = ((lane % n_sp == sp) & (lane < 3 * n_sp)).astype(f32)

    steps = 2 * nz
    before, after = {}, {}

    def put(table, s, work, *args):
        table.setdefault(s, []).append(functools.partial(work, *args))

    end = nz - 1
    for k in range(1, nz):
        put(before, 2 * k - 1, relay, k)
        if k < end:
            put(before, 2 * k, take, k + 1)
        put(before, 2 * k, sides, k)
        put(before, 2 * k, corner, k)
    for k in range(end - 1):
        put(after, 2 * k + 2, merge, k)
        if k > 0:
            put(before, 2 * k + 3, stage1, k)
    put(before, 2 * end, merge, end - 1)
    put(before, 2 * end, stage1, end - 1)
    put(before, 2 * end + 1, stage2, 1)

    @pl.loop(0, steps)
    def _(s):
        for at, works in before.items():
            @pl.when(s == at)
            def _():
                for work in works:
                    work()

        k = s // 2
        shared = (s + k // (nz - 1)) % 2
        core = (c + shared) % 2
        at_z = jnp.where(k < 2, 2 * (z // 2) + (z + k) % 2, k + (z // 2) * (nz - 1 - 2 * k))
        i = pl.ds(at_z * n_sp, n_sp)

        @pl.when(shared == 1)
        def _():
            for rel in range(n_sp):
                at = xbuf.at[1 - c, at_z * n_sp + rel]
                n = k * n_sp + rel
                rc(at, at, s_p.at[n], r_p.at[n], other).wait_recv()

        held = xbuf[core, i].reshape(n_sp * rows, xbuf.shape[3])
        scale = jnp.sum(held[:, width:].astype(f32) * chosen, axis=1, keepdims=True)
        held = held[:, :width]
        gate = jnp.dot(held, wg[...], preferred_element_type=f32)
        up = jnp.dot(held, wu[...], preferred_element_type=f32)
        act = (jax.nn.silu(gate) * up * scale).astype(jnp.bfloat16)
        down = jnp.dot(act, wd[...], preferred_element_type=f32)
        pbuf[core, i] = down.astype(pbuf.dtype).reshape(n_sp, rows, width)

        @pl.when(shared == 1)
        def _():
            rc(pbuf.at[1 - c, i], dbuf.at[i], s_d.at[k], r_d.at[k], other).start()

        for at, works in after.items():
            @pl.when(s == at)
            def _():
                for work in works:
                    work()

    merge(end)
    stage1(end)
    for k in range(2, end):
        stage2(k)
    stage1(0, (1,))
    stage3(1)
    stage2(end)
    stage1(0, (0,))
    for k in range(2, end):
        stage3(k)
    stage3(end)
    stage2(0)
    for h in (0, 1):
        total = summed(h, 0)
        for k in range(1, nz):
            if h == 0:
                rz_recv(k).wait_recv()
            total = total + rz[zz(k), :, cols(h)].astype(f32)
        out_ref[:, cols(h)] = (hid[:, cols(h)].astype(f32) + total).astype(out_ref.dtype)

    for copy in halo_copies():
        copy.wait_send()
    for d in range(1, n_tp):
        @pl.when(lax.rem(tp + d, n_tp) != 0)
        def _():
            swap(d).wait_send()

    @pl.when(tp != 0)
    def _():
        swap_first().wait_send()

    for k in range(1, nz):
        z_send(k).wait_send()
        rz_copy(k).wait_send()
    for k in range(nz):
        for h in (0, 1):
            first(h, k).wait_send()
            second(h, k).wait_send()
            third(h, k).wait_send()
            r1_copy(h, 0, k).wait_send()
            r1_copy(h, 1, k).wait_send()
            r2_copy(h, k).wait_send()
        for rel in range(n_sp):
            to_other(rel, k).wait_send()
    for k in range(nz):
        d_copy(k).wait_send()


def layer(gate_b, gate_c, values_in, conv_w, docs, resid, gain, ids, route, w_out, w_gate, w_up, w_down):
    rows, width = resid.shape
    wide = width + LANES
    seq, held = gate_b.shape
    n_tp = lax.axis_size("tp")
    n_sp = lax.axis_size("sp")
    nz = n_tp // 2
    half = width // 2
    bf = jnp.bfloat16
    f32 = jnp.float32
    dma = pltpu.SemaphoreType.DMA
    hbm = pl.BlockSpec(memory_space=pl.ANY)
    vmem = pl.BlockSpec(memory_space=pltpu.VMEM)
    operands = (gate_b, gate_c, values_in, conv_w, docs, resid, gain, ids, route)
    return pl.pallas_call(
        moe_kernel,
        out_shape=jax.ShapeDtypeStruct((rows, width), bf),
        in_specs=[hbm] * 13,
        out_specs=vmem,
        scratch_shapes=[pltpu.VMEM(a.shape, a.dtype) for a in operands] + [
            pltpu.VMEM((rows, width), bf),
            pltpu.VMEM((rows, n_tp * held), bf),
            pltpu.VMEM((seq, held), bf),
            pltpu.VMEM((seq + 8, held), f32),
            pltpu.VMEM((seq + 8, held), f32),
            pltpu.VMEM((LANES, LANES), f32),
            pltpu.VMEM((16, held), bf),
            pltpu.VMEM((16, held), bf),
            pltpu.VMEM(docs.shape, docs.dtype),
            pltpu.VMEM(w_out.shape, bf),
            pltpu.VMEM((2, n_sp * nz, rows, wide), bf),
            pltpu.VMEM((2, n_sp * nz, rows, width), bf),
            pltpu.VMEM((n_sp * nz, rows, width), bf),
            pltpu.VMEM((2, 2, nz, rows, half), bf),
            pltpu.VMEM((2, nz, rows, half), bf),
            pltpu.VMEM((nz, rows, width), bf),
            pltpu.VMEM(w_gate.shape, bf),
            pltpu.VMEM(w_up.shape, bf),
            pltpu.VMEM(w_down.shape, bf),
            dma((9,)), dma((4,)),
            dma((n_tp,)), dma((n_tp,)), dma, dma((3,)), dma((3,)),
            dma((nz,)), dma((nz,)), dma((2, nz)), dma((2, 2, nz)), dma((2, 4, nz)),
            dma((n_sp * nz,)), dma((n_sp * nz,)),
            dma((nz,)), dma((nz,)),
            dma((2, 2, nz)), dma((2, 2, nz)), dma((2, nz)), dma((2, nz)),
            dma((nz,)), dma((nz,)),
        ],
        compiler_params=pltpu.CompilerParams(
            collective_id=0, has_side_effects=True, vmem_limit_bytes=64000000
        ),
    )(*operands, w_out, w_gate, w_up, w_down)


def passed_along(block, axis, distance):
    devices = range(lax.axis_size(axis))
    route = [(i - distance, i) for i in devices if i - distance in devices]
    return lax.ppermute(block, axis, route)


def local(
    gate_b,
    gate_c,
    values_in,
    conv_w,
    documents,
    w_out,
    resid,
    norm_gain,
    route_ids,
    route_weight,
    w_gate,
    w_up,
    w_down,
):
    seq_rows = gate_b.shape[0]
    local_rows = resid.shape[0]
    model_width = resid.shape[1]
    experts = lax.axis_size("sp") * w_gate.shape[0]
    capacity = 4 * local_rows // experts
    if lax.axis_size("sp") == 4 and w_gate.shape[0] == 1 and capacity >= local_rows:
        return layer(
            gate_b, gate_c, values_in, conv_w, documents.reshape(-1, LANES), resid,
            norm_gain.reshape(-1, LANES), route_ids.T, route_weight.T,
            w_out, w_gate[0], w_up[0], w_down[0],
        )
    last_rows = jnp.stack([gate_c[seq_rows - 2 :], values_in[seq_rows - 2 :]])
    before, before_docs = passed_along((last_rows, documents[seq_rows - 2 :]), "sp", 1)
    products = jnp.concatenate(
        [
            before[0].astype(jnp.float32) * before[1].astype(jnp.float32),
            gate_c.astype(jnp.float32) * values_in.astype(jnp.float32),
        ],
        axis=0,
    )
    docs_all = jnp.concatenate([before_docs, documents], axis=0)
    kernel_taps = conv_w.astype(jnp.float32)
    near_mask = (docs_all[1:-1] == documents).astype(jnp.float32)[:, None]
    far_mask = (docs_all[:-2] == documents).astype(jnp.float32)[:, None]
    convolved = (
        kernel_taps[2] * products[2:]
        + kernel_taps[1] * products[1:-1] * near_mask
        + kernel_taps[0] * products[:-2] * far_mask
    )
    mixed_rows = (gate_b.astype(jnp.float32) * convolved).astype(jnp.bfloat16)
    token_rows = lax.all_to_all(mixed_rows, "tp", split_axis=0, concat_axis=1, tiled=True)
    projected = jnp.dot(token_rows, w_out, preferred_element_type=jnp.float32)
    hidden_state = (resid.astype(jnp.float32) + projected).astype(jnp.bfloat16)
    state_wide = hidden_state.astype(jnp.float32)
    normed = (
        state_wide
        * lax.rsqrt(jnp.mean(state_wide * state_wide, axis=-1, keepdims=True) + 1e-06)
        * norm_gain.astype(jnp.float32)
    ).astype(jnp.bfloat16)
    experts = lax.axis_size("sp") * w_gate.shape[0]
    capacity = 4 * local_rows // experts
    flat_ids = route_ids.reshape(-1)
    one_hot = (flat_ids[:, None] == jnp.arange(experts, dtype=jnp.int32)[None, :]).astype(jnp.int32)
    rank_in = jnp.sum((jnp.cumsum(one_hot, axis=0) - one_hot) * one_hot, axis=1)
    slot_index = flat_ids * capacity + rank_in
    placement = (
        slot_index[:, None] == jnp.arange(experts * capacity, dtype=jnp.int32)[None, :]
    ).astype(jnp.bfloat16)
    repeated = jnp.repeat(normed, 2, axis=0)
    dispatch = jnp.einsum(
        "js,jd->sd", placement, repeated, preferred_element_type=jnp.float32
    ).astype(jnp.bfloat16)
    dispatch = dispatch.reshape(experts, capacity, model_width)
    gathered_piece = lax.all_gather(
        lax.all_to_all(dispatch, "sp", split_axis=0, concat_axis=0, tiled=True),
        "tp",
        axis=0,
        tiled=True,
    )
    flat_rows = gathered_piece.reshape(-1, model_width)
    gate_part = jnp.dot(flat_rows, w_gate[0], preferred_element_type=jnp.float32)
    up_part = jnp.dot(flat_rows, w_up[0], preferred_element_type=jnp.float32)
    activated = (jax.nn.silu(gate_part) * up_part).astype(jnp.bfloat16)
    partial_value = jnp.dot(activated, w_down[0], preferred_element_type=jnp.float32)
    partial_value = partial_value.reshape(
        gathered_piece.shape[0], gathered_piece.shape[1], model_width
    )
    summed = lax.psum_scatter(
        partial_value.astype(jnp.bfloat16), "tp", scatter_dimension=0, tiled=True
    )
    returned = lax.all_to_all(summed, "sp", split_axis=0, concat_axis=0, tiled=True)
    picked = jnp.take(
        returned.reshape(experts * capacity, model_width), slot_index, axis=0
    ).reshape(local_rows, 2, model_width)
    combined = jnp.sum(route_weight[:, :, None] * picked.astype(jnp.float32), axis=1)
    return (hidden_state.astype(jnp.float32) + combined).astype(jnp.bfloat16)


def solution(mesh):
    return jax.shard_map(
        local,
        mesh=mesh,
        in_specs=(
            P("sp", "tp"),
            P("sp", "tp"),
            P("sp", "tp"),
            P(None, "tp"),
            P("sp"),
            P(),
            P(("sp", "tp"), None),
            P(),
            P(("sp", "tp"), None),
            P(("sp", "tp"), None),
            P("sp", None, "tp"),
            P("sp", None, "tp"),
            P("sp", "tp", None),
        ),
        out_specs=P(("sp", "tp"), None),
        check_vma=False,
    )
```

```python
import functools

import jax
import jax.numpy as jnp
from jax import lax
from jax.experimental import pallas as pl
from jax.experimental.pallas import tpu as pltpu
from jax.sharding import PartitionSpec as P

MESH = pl.DeviceIdType.MESH
LANES = 128


def moe_kernel(
    gb_hbm, gc_hbm, vals_hbm, taps_hbm, docs_hbm, resid_hbm, gain_hbm, ids_hbm, route_hbm,
    wo_hbm, wg_hbm, wu_hbm, wd_hbm, out_ref,
    gb, gc, vals, taps, docs, resid, gain, ids, route,
    hid, tok, mixed, pad, dpad, mat, hc, hv, hd, wo,
    xbuf, pbuf, dbuf, r1, r2, rm, rz, wg, wu, wd,
    in_sem, w_sem,
    s_a, r_a, s_b, s_h, r_h3,
    s_z, s_f, r_z, s_1, s_2, r_h, s_p, r_p,
    s_d, r_d, s_r1, r_r1, s_r2, r_r2, s_m, r_m, s_rz, r_rz,
):
    f32 = jnp.float32
    n_sp, n_tp = lax.axis_size("sp"), lax.axis_size("tp")
    nz = n_tp // 2
    width = out_ref.shape[1]
    half = width // 2
    rows = out_ref.shape[0]
    seq = gb.shape[0]
    halo = hc.shape[0]
    sp, tp = lax.axis_index("sp"), lax.axis_index("tp")
    y, x = sp // 2, sp % 2
    z, c = tp // 2, tp % 2
    xn, yn, dg = y * 2 + 1 - x, (1 - y) * 2 + x, (1 - y) * 2 + 1 - x
    columns = (sp, xn, yn, dg)
    OWN, XN, YN, DG = range(4)
    other = (sp, z * 2 + 1 - c)
    following, previous = (lax.rem(sp + 1, n_sp), tp), (lax.rem(sp + n_sp - 1, n_sp), tp)
    to_x, to_y = (xn, tp), (yn, tp)
    inner = z % 2 != z // 2
    outer = z % 2 == z // 2

    def zz(k):
        if k < 2:
            return 2 * (z // 2) + (z + k) % 2
        return k + (z // 2) * (nz - 1 - 2 * k)

    def slot(k, rel):
        return zz(k) * n_sp + columns[rel]

    def lanes(h):
        return pl.ds(0, half) if h == 0 else pl.ds(half, xbuf.shape[3] - half)

    def cols(h):
        return pl.ds(h * half, half)

    def rc(src, dst, ss, rs, dev):
        return pltpu.make_async_remote_copy(
            src_ref=src, dst_ref=dst, send_sem=ss, recv_sem=rs,
            device_id=dev, device_id_type=MESH,
        )


    def halo_copies():
        pairs = (
            (gc.at[pl.ds(seq - halo, halo)], hc),
            (vals.at[pl.ds(seq - halo, halo)], hv),
            (docs, hd),
        )
        return [rc(a, b, s_h.at[n], r_h3.at[n], following) for n, (a, b) in enumerate(pairs)]

    def channels(j):
        return pl.ds(pl.multiple_of(j * gb.shape[1], gb.shape[1]), gb.shape[1])

    def token_rows(j):
        return mixed.at[pl.ds(pl.multiple_of(j * rows, rows), rows)]

    def swap(d):
        j = lax.rem(tp + d, n_tp)
        return rc(token_rows(j), tok.at[:, channels(tp)], s_a.at[d], r_a.at[tp], (sp, j))

    def swapped(d):
        j = lax.rem(tp + d, n_tp)
        return rc(token_rows(j), tok.at[:, channels(j)], s_a.at[d], r_a.at[j], (sp, j))

    def swap_first():
        return rc(token_rows(0), tok.at[:, channels(tp)], s_b, r_a.at[tp], (sp, 0))

    def convolve(first, count):
        own = pl.ds(first, count)
        now = dpad[pl.ds(first + 8, count)]
        near = (dpad[pl.ds(first + 7, count)] == now).astype(f32)
        far = (dpad[pl.ds(first + 6, count)] == now).astype(f32)
        tap = taps[...].astype(f32)
        convolved = (
            tap[2:3] * pad[pl.ds(first + 8, count)]
            + tap[1:2] * pad[pl.ds(first + 7, count)] * near
            + tap[0:1] * pad[pl.ds(first + 6, count)] * far
        )
        mixed[own] = (gb[own].astype(f32) * convolved).astype(mixed.dtype)

    def mix():
        mat[...] = jnp.zeros_like(mat)
        doc_rows = docs.shape[0]
        mat[pl.ds(0, doc_rows)] = docs[...].astype(f32)
        mat[pl.ds(doc_rows, 2), pl.ds(0, rows)] = ids[...].astype(f32)
        mat[pl.ds(doc_rows + 2, 2), pl.ds(0, rows)] = route[...]
        turned = mat[...].T
        for n in range(doc_rows):
            dpad[pl.ds(8 + n * LANES, LANES)] = jnp.broadcast_to(
                turned[:, n : n + 1], (LANES, dpad.shape[1])
            )
        pad[pl.ds(8, seq)] = gc[...].astype(f32) * vals[...].astype(f32)
        pad[pl.ds(0, 8)] = jnp.zeros((8, pad.shape[1]), f32)
        dpad[pl.ds(0, 8)] = jnp.full((8, dpad.shape[1]), -1.0, f32)
        convolve(0, seq)
        for d in range(1, n_tp):
            @pl.when(lax.rem(tp + d, n_tp) != 0)
            def _():
                swap(d).start()

        lane = lax.broadcasted_iota(jnp.int32, (rows, LANES), 1)
        named = (lane % n_sp).astype(f32)
        part = lane // n_sp
        side = turned[:rows]
        at = doc_rows
        share = jnp.where(side[:, at : at + 1] == named, side[:, at + 2 : at + 3], 0.0) + jnp.where(
            side[:, at + 1 : at + 2] == named, side[:, at + 3 : at + 4], 0.0
        )
        high = share.astype(jnp.bfloat16).astype(f32)
        middle = (share - high).astype(jnp.bfloat16).astype(f32)
        low = share - high - middle
        terms = jnp.where(part == 0, high, jnp.where(part == 1, middle, jnp.where(part == 2, low, 0.0)))
        mine = z * n_sp + sp
        xbuf[c, mine, :, pl.ds(width, LANES)] = terms.astype(xbuf.dtype)

        for copy in halo_copies():
            copy.wait_recv()
        pad[pl.ds(0, 8)] = (hc[...].astype(f32) * hv[...].astype(f32))[halo - 8 :]
        last = hd[pl.ds(doc_rows - 1, 1)].astype(f32)
        last = jnp.where(sp == 0, -1.0, last)
        for n in (1, 2):
            dpad[pl.ds(8 - n, 1)] = jnp.broadcast_to(
                last[:, LANES - n : LANES - n + 1], (1, dpad.shape[1])
            )
        convolve(0, 16)

        @pl.when(tp != 0)
        def _():
            swap_first().start()

        tok[:, channels(tp)] = mixed[pl.ds(pl.multiple_of(tp * rows, rows), rows)]
        in_copies[5].wait()
        in_copies[6].wait()
        wo_copy.wait()
        for d in range(1, n_tp):
            swapped(d).wait_recv()
        projected = jnp.dot(tok[...], wo[...], preferred_element_type=f32)
        hidden = (resid[...].astype(f32) + projected).astype(hid.dtype)
        hid[...] = hidden
        state = hidden.astype(f32)
        scale = lax.rsqrt(jnp.mean(state * state, axis=-1, keepdims=True) + 1e-06)
        for n in range(width // LANES):
            at = slice(n * LANES, (n + 1) * LANES)
            xbuf[c, mine, :, pl.ds(n * LANES, LANES)] = (
                state[:, at] * scale * gain[n : n + 1].astype(f32)
            ).astype(xbuf.dtype)


    def z_send(k):
        at = xbuf.at[c, z * n_sp + sp]
        return rc(at, at, s_z.at[k], r_z.at[z], (sp, zz(k) * 2 + c))

    def z_recv(k):
        at = xbuf.at[c, slot(k, OWN)]
        return rc(at, at, s_z.at[k], r_z.at[zz(k)], (sp, zz(k) * 2 + c))

    def forward(k):
        at = xbuf.at[c, slot(k, OWN)]
        return rc(at, at, s_f.at[k], r_z.at[zz(k)], (sp, zz(2 if k == 1 else 1) * 2 + c))

    def pass_on(k):
        @pl.when(inner)
        def _():
            if k > 1:
                z_recv(k).wait_recv()
            forward(k).start()

    def piece(h, rel, k, ss, there, dev):
        at = xbuf.at[c, slot(k, rel), :, lanes(h)]
        return rc(at, at, ss, r_h.at[h, there, k], dev)

    def first(h, k):
        return piece(h, OWN, k, s_1.at[h, k], YN if h == 0 else XN, to_y if h == 0 else to_x)

    def second(h, k):
        return piece(h, OWN, k, s_2.at[h, 0, k], XN if h == 0 else YN, to_x if h == 0 else to_y)

    def third(h, k):
        return piece(h, YN if h == 0 else XN, k, s_2.at[h, 1, k], DG, to_x if h == 0 else to_y)

    def arrived(h, rel, k):
        piece(h, rel, k, s_1.at[h, k], rel, other).wait_recv()

    def to_other(rel, k):
        at = xbuf.at[c, slot(k, rel)]
        return rc(at, at, s_p.at[k * n_sp + rel], r_p.at[k * n_sp + rel], other)

    def spread(k):
        for h in (1, 0):
            first(h, k).start()
        for h in (0, 1):
            second(h, k).start()
        to_other(OWN, k).start()

    def take(k):
        if k == 1:
            z_recv(k).wait_recv()
        else:
            @pl.when(outer)
            def _():
                z_recv(k).wait_recv()
        spread(k)

    def relay(k):
        arrived(0, YN, k)
        third(0, k).start()
        arrived(1, XN, k)
        third(1, k).start()

    def sides(k):
        arrived(0, XN, k)
        to_other(XN, k).start()
        arrived(1, YN, k)
        to_other(YN, k).start()

    def corner(k):
        arrived(0, DG, k)
        arrived(1, DG, k)
        to_other(DG, k).start()


    def group(k):
        return pl.ds(zz(k) * n_sp, n_sp)

    def d_copy(k):
        return rc(pbuf.at[1 - c, group(k)], dbuf.at[group(k)], s_d.at[k], r_d.at[k], other)

    def merge(k):
        d_copy(k).wait_recv()
        i = group(k)
        pbuf[c, i] = (pbuf[c, i].astype(f32) + dbuf[i].astype(f32)).astype(pbuf.dtype)

    def r1_copy(h, o, k):
        rel = DG if o else (XN if h == 0 else YN)
        at = pbuf.at[c, slot(k, rel), :, cols(h)]
        return rc(at, r1.at[h, o, k], s_r1.at[h, o, k], r_r1.at[h, o, k], to_x if h == 0 else to_y)

    def r2_copy(h, k):
        at = pbuf.at[c, slot(k, YN if h == 0 else XN), :, cols(h)]
        return rc(at, r2.at[h, k], s_r2.at[h, k], r_r2.at[h, k], to_y if h == 0 else to_x)

    def mate_copy(k):
        at = pbuf.at[c, slot(k, OWN)]
        return rc(at, rm.at[k - 2], s_m.at[k - 2], r_m.at[k - 2], (sp, zz(1) * 2 + c))

    def rz_copy(k):
        n = min(k - 1, 1)
        at = pbuf.at[c, slot(k, OWN)]
        return rc(at, rz.at[n], s_rz.at[k], r_rz.at[n], (sp, zz(k) * 2 + c))

    def stage1(k, parts=(1, 0)):
        for o in parts:
            for h in (0, 1):
                r1_copy(h, o, k).start()

    def stage2(k):
        for h in (0, 1):
            r1_copy(h, 1, k).wait_recv()
            i = slot(k, YN if h == 0 else XN)
            pbuf[c, i, :, cols(h)] = (
                pbuf[c, i, :, cols(h)].astype(f32) + r1[h, 1, k].astype(f32)
            ).astype(pbuf.dtype)
            r2_copy(h, k).start()

    def summed(h, k):
        r1_copy(h, 0, k).wait_recv()
        r2_copy(h, k).wait_recv()
        return (
            pbuf[c, slot(k, OWN), :, cols(h)].astype(f32)
            + r1[h, 0, k].astype(f32)
            + r2[h, k].astype(f32)
        )

    def stage3(k):
        for h in (0, 1):
            pbuf[c, slot(k, OWN), :, cols(h)] = summed(h, k).astype(pbuf.dtype)
        if k == 1:
            rz_copy(k).start()
        else:
            @pl.when(outer)
            def _():
                mate_copy(k).start()

    def stage4(k):
        @pl.when(inner)
        def _():
            mate_copy(k).wait_recv()
            at = slot(k, OWN)
            pbuf[c, at] = (pbuf[c, at].astype(f32) + rm[k - 2].astype(f32)).astype(pbuf.dtype)
            rz_copy(k).start()

    barrier = pltpu.get_barrier_semaphore()
    peers = [to_x, to_y, following, previous] + [(sp, lax.rem(tp + d, n_tp)) for d in range(1, n_tp)]
    for peer in peers:
        pl.semaphore_signal(barrier, inc=1, device_id=peer, device_id_type=MESH)
    in_copies = [
        pltpu.make_async_copy(a, b, in_sem.at[n])
        for n, (a, b) in enumerate((
            (gc_hbm, gc), (vals_hbm, vals), (docs_hbm, docs), (taps_hbm, taps), (gb_hbm, gb),
            (resid_hbm, resid), (gain_hbm, gain), (ids_hbm, ids), (route_hbm, route),
        ))
    ]
    weights = [
        pltpu.make_async_copy(a, b, w_sem.at[n])
        for n, (a, b) in enumerate(((wg_hbm, wg), (wu_hbm, wu), (wd_hbm, wd)))
    ]
    wo_copy = pltpu.make_async_copy(wo_hbm, wo, w_sem.at[3])
    for copy in in_copies:
        copy.start()
    wo_copy.start()
    for w in weights:
        w.start()
    for n in (0, 1, 2):
        in_copies[n].wait()
    pl.semaphore_wait(barrier, len(peers))
    for copy in halo_copies():
        copy.start()
    for n in (3, 4, 7, 8):
        in_copies[n].wait()
    mix()
    for h in (1, 0):
        first(h, 0).start()
    z_send(1).start()

    @pl.when(inner)
    def _():
        z_send(2).start()

    for h in (0, 1):
        second(h, 0).start()
    to_other(OWN, 0).start()
    relay(0)
    take(1)
    pass_on(1)
    pass_on(2)
    sides(0)
    corner(0)
    for w in weights:
        w.wait()

    lane = lax.broadcasted_iota(jnp.int32, (1, LANES), 1)
    chosen = ((lane % n_sp == sp) & (lane < 3 * n_sp)).astype(f32)

    steps = 2 * nz
    before, after = {}, {}

    def put(table, s, work, *args):
        table.setdefault(s, []).append(functools.partial(work, *args))

    end = nz - 1
    put(before, 2, pass_on, 3)
    for k in range(1, nz):
        put(before, 2 * k - 1, relay, k)
        if k < end:
            put(before, 2 * k, take, k + 1)
        put(before, 2 * k, sides, k)
        put(before, 2 * k, corner, k)
    for k in range(end - 1):
        put(after, 2 * k + 2, merge, k)
    put(before, 2 * end - 1, stage1, 1, (1,))
    put(before, 2 * end, merge, end - 1)
    put(before, 2 * end, stage1, end - 1)
    put(before, 2 * end + 1, stage2, end - 1)

    @pl.loop(0, steps)
    def _(s):
        for at, works in before.items():
            @pl.when(s == at)
            def _():
                for work in works:
                    work()

        k = s // 2
        shared = (s + k // (nz - 1)) % 2
        core = (c + shared) % 2
        at_z = jnp.where(k < 2, 2 * (z // 2) + (z + k) % 2, k + (z // 2) * (nz - 1 - 2 * k))
        i = pl.ds(at_z * n_sp, n_sp)

        @pl.when(shared == 1)
        def _():
            for rel in range(n_sp):
                at = xbuf.at[1 - c, at_z * n_sp + rel]
                n = k * n_sp + rel
                rc(at, at, s_p.at[n], r_p.at[n], other).wait_recv()

        held = xbuf[core, i].reshape(n_sp * rows, xbuf.shape[3])
        scale = jnp.sum(held[:, width:].astype(f32) * chosen, axis=1, keepdims=True)
        held = held[:, :width]
        gate = jnp.dot(held, wg[...], preferred_element_type=f32)
        up = jnp.dot(held, wu[...], preferred_element_type=f32)
        act = (jax.nn.silu(gate) * up * scale).astype(jnp.bfloat16)
        down = jnp.dot(act, wd[...], preferred_element_type=f32)
        pbuf[core, i] = down.astype(pbuf.dtype).reshape(n_sp, rows, width)

        @pl.when(shared == 1)
        def _():
            rc(pbuf.at[1 - c, i], dbuf.at[i], s_d.at[k], r_d.at[k], other).start()

        for at, works in after.items():
            @pl.when(s == at)
            def _():
                for work in works:
                    work()

    merge(end)
    stage1(end)
    stage3(end - 1)
    stage2(end)
    stage1(1, (0,))
    stage2(1)
    stage1(0)
    stage4(end - 1)
    stage3(end)
    stage3(1)
    stage4(end)
    stage2(0)
    rz_copy(1).wait_recv()
    rz_copy(2).wait_recv()
    for h in (0, 1):
        total = summed(h, 0) + rz[0, :, cols(h)].astype(f32) + rz[1, :, cols(h)].astype(f32)
        out_ref[:, cols(h)] = (hid[:, cols(h)].astype(f32) + total).astype(out_ref.dtype)

    for copy in halo_copies():
        copy.wait_send()
    for d in range(1, n_tp):
        @pl.when(lax.rem(tp + d, n_tp) != 0)
        def _():
            swap(d).wait_send()

    @pl.when(tp != 0)
    def _():
        swap_first().wait_send()

    z_send(1).wait_send()
    rz_copy(1).wait_send()

    @pl.when(inner)
    def _():
        z_send(2).wait_send()
        for k in range(1, nz):
            forward(k).wait_send()
        for k in range(2, nz):
            rz_copy(k).wait_send()

    @pl.when(outer)
    def _():
        for k in range(2, nz):
            mate_copy(k).wait_send()

    for k in range(nz):
        for h in (0, 1):
            first(h, k).wait_send()
            second(h, k).wait_send()
            third(h, k).wait_send()
            r1_copy(h, 0, k).wait_send()
            r1_copy(h, 1, k).wait_send()
            r2_copy(h, k).wait_send()
        for rel in range(n_sp):
            to_other(rel, k).wait_send()
    for k in range(nz):
        d_copy(k).wait_send()


def layer(gate_b, gate_c, values_in, conv_w, docs, resid, gain, ids, route, w_out, w_gate, w_up, w_down):
    rows, width = resid.shape
    wide = width + LANES
    seq, held = gate_b.shape
    n_tp = lax.axis_size("tp")
    n_sp = lax.axis_size("sp")
    nz = n_tp // 2
    half = width // 2
    bf = jnp.bfloat16
    f32 = jnp.float32
    dma = pltpu.SemaphoreType.DMA
    hbm = pl.BlockSpec(memory_space=pl.ANY)
    vmem = pl.BlockSpec(memory_space=pltpu.VMEM)
    operands = (gate_b, gate_c, values_in, conv_w, docs, resid, gain, ids, route)
    return pl.pallas_call(
        moe_kernel,
        out_shape=pltpu.VMEM((rows, width), bf),
        in_specs=[hbm] * 13,
        out_specs=vmem,
        scratch_shapes=[pltpu.VMEM(a.shape, a.dtype) for a in operands] + [
            pltpu.VMEM((rows, width), bf),
            pltpu.VMEM((rows, n_tp * held), bf),
            pltpu.VMEM((seq, held), bf),
            pltpu.VMEM((seq + 8, held), f32),
            pltpu.VMEM((seq + 8, held), f32),
            pltpu.VMEM((LANES, LANES), f32),
            pltpu.VMEM((16, held), bf),
            pltpu.VMEM((16, held), bf),
            pltpu.VMEM(docs.shape, docs.dtype),
            pltpu.VMEM(w_out.shape, bf),
            pltpu.VMEM((2, n_sp * nz, rows, wide), bf),
            pltpu.VMEM((2, n_sp * nz, rows, width), bf),
            pltpu.VMEM((n_sp * nz, rows, width), bf),
            pltpu.VMEM((2, 2, nz, rows, half), bf),
            pltpu.VMEM((2, nz, rows, half), bf),
            pltpu.VMEM((2, rows, width), bf),
            pltpu.VMEM((2, rows, width), bf),
            pltpu.VMEM(w_gate.shape, bf),
            pltpu.VMEM(w_up.shape, bf),
            pltpu.VMEM(w_down.shape, bf),
            dma((9,)), dma((4,)),
            dma((n_tp,)), dma((n_tp,)), dma, dma((3,)), dma((3,)),
            dma((nz,)), dma((nz,)), dma((nz,)), dma((2, nz)), dma((2, 2, nz)), dma((2, 4, nz)),
            dma((n_sp * nz,)), dma((n_sp * nz,)),
            dma((nz,)), dma((nz,)),
            dma((2, 2, nz)), dma((2, 2, nz)), dma((2, nz)), dma((2, nz)),
            dma((2,)), dma((2,)), dma((nz,)), dma((2,)),
        ],
        compiler_params=pltpu.CompilerParams(
            collective_id=0, has_side_effects=True, vmem_limit_bytes=64000000
        ),
    )(*operands, w_out, w_gate, w_up, w_down)


def passed_along(block, axis, distance):
    devices = range(lax.axis_size(axis))
    route = [(i - distance, i) for i in devices if i - distance in devices]
    return lax.ppermute(block, axis, route)


def local(
    gate_b,
    gate_c,
    values_in,
    conv_w,
    documents,
    w_out,
    resid,
    norm_gain,
    route_ids,
    route_weight,
    w_gate,
    w_up,
    w_down,
):
    seq_rows = gate_b.shape[0]
    local_rows = resid.shape[0]
    model_width = resid.shape[1]
    experts = lax.axis_size("sp") * w_gate.shape[0]
    capacity = 4 * local_rows // experts
    if (lax.axis_size("sp"), lax.axis_size("tp")) == (4, 8) and w_gate.shape[0] == 1 and capacity >= local_rows:
        return layer(
            gate_b, gate_c, values_in, conv_w, documents.reshape(-1, LANES), resid,
            norm_gain.reshape(-1, LANES), route_ids.T, route_weight.T,
            w_out, w_gate[0], w_up[0], w_down[0],
        )
    last_rows = jnp.stack([gate_c[seq_rows - 2 :], values_in[seq_rows - 2 :]])
    before, before_docs = passed_along((last_rows, documents[seq_rows - 2 :]), "sp", 1)
    products = jnp.concatenate(
        [
            before[0].astype(jnp.float32) * before[1].astype(jnp.float32),
            gate_c.astype(jnp.float32) * values_in.astype(jnp.float32),
        ],
        axis=0,
    )
    docs_all = jnp.concatenate([before_docs, documents], axis=0)
    kernel_taps = conv_w.astype(jnp.float32)
    near_mask = (docs_all[1:-1] == documents).astype(jnp.float32)[:, None]
    far_mask = (docs_all[:-2] == documents).astype(jnp.float32)[:, None]
    convolved = (
        kernel_taps[2] * products[2:]
        + kernel_taps[1] * products[1:-1] * near_mask
        + kernel_taps[0] * products[:-2] * far_mask
    )
    mixed_rows = (gate_b.astype(jnp.float32) * convolved).astype(jnp.bfloat16)
    token_rows = lax.all_to_all(mixed_rows, "tp", split_axis=0, concat_axis=1, tiled=True)
    projected = jnp.dot(token_rows, w_out, preferred_element_type=jnp.float32)
    hidden_state = (resid.astype(jnp.float32) + projected).astype(jnp.bfloat16)
    state_wide = hidden_state.astype(jnp.float32)
    normed = (
        state_wide
        * lax.rsqrt(jnp.mean(state_wide * state_wide, axis=-1, keepdims=True) + 1e-06)
        * norm_gain.astype(jnp.float32)
    ).astype(jnp.bfloat16)
    experts = lax.axis_size("sp") * w_gate.shape[0]
    capacity = 4 * local_rows // experts
    flat_ids = route_ids.reshape(-1)
    one_hot = (flat_ids[:, None] == jnp.arange(experts, dtype=jnp.int32)[None, :]).astype(jnp.int32)
    rank_in = jnp.sum((jnp.cumsum(one_hot, axis=0) - one_hot) * one_hot, axis=1)
    slot_index = flat_ids * capacity + rank_in
    placement = (
        slot_index[:, None] == jnp.arange(experts * capacity, dtype=jnp.int32)[None, :]
    ).astype(jnp.bfloat16)
    repeated = jnp.repeat(normed, 2, axis=0)
    dispatch = jnp.einsum(
        "js,jd->sd", placement, repeated, preferred_element_type=jnp.float32
    ).astype(jnp.bfloat16)
    dispatch = dispatch.reshape(experts, capacity, model_width)
    gathered_piece = lax.all_gather(
        lax.all_to_all(dispatch, "sp", split_axis=0, concat_axis=0, tiled=True),
        "tp",
        axis=0,
        tiled=True,
    )
    flat_rows = gathered_piece.reshape(-1, model_width)
    gate_part = jnp.dot(flat_rows, w_gate[0], preferred_element_type=jnp.float32)
    up_part = jnp.dot(flat_rows, w_up[0], preferred_element_type=jnp.float32)
    activated = (jax.nn.silu(gate_part) * up_part).astype(jnp.bfloat16)
    partial_value = jnp.dot(activated, w_down[0], preferred_element_type=jnp.float32)
    partial_value = partial_value.reshape(
        gathered_piece.shape[0], gathered_piece.shape[1], model_width
    )
    summed = lax.psum_scatter(
        partial_value.astype(jnp.bfloat16), "tp", scatter_dimension=0, tiled=True
    )
    returned = lax.all_to_all(summed, "sp", split_axis=0, concat_axis=0, tiled=True)
    picked = jnp.take(
        returned.reshape(experts * capacity, model_width), slot_index, axis=0
    ).reshape(local_rows, 2, model_width)
    combined = jnp.sum(route_weight[:, :, None] * picked.astype(jnp.float32), axis=1)
    return (hidden_state.astype(jnp.float32) + combined).astype(jnp.bfloat16)


def solution(mesh):
    return jax.shard_map(
        local,
        mesh=mesh,
        in_specs=(
            P("sp", "tp"),
            P("sp", "tp"),
            P("sp", "tp"),
            P(None, "tp"),
            P("sp"),
            P(),
            P(("sp", "tp"), None),
            P(),
            P(("sp", "tp"), None),
            P(("sp", "tp"), None),
            P("sp", None, "tp"),
            P("sp", None, "tp"),
            P("sp", "tp", None),
        ),
        out_specs=P(("sp", "tp"), None),
        check_vma=False,
    )
```

```python
import functools

import jax
import jax.numpy as jnp
from jax import lax
from jax.experimental import pallas as pl
from jax.experimental.pallas import tpu as pltpu
from jax.sharding import PartitionSpec as P

MESH = pl.DeviceIdType.MESH
LANES = 128


def moe_kernel(
    gb_hbm, gc_hbm, vals_hbm, taps_hbm, docs_hbm, resid_hbm, gain_hbm, ids_hbm, route_hbm,
    wo_hbm, wg_hbm, wu_hbm, wd_hbm, out_ref,
    gb, gc, vals, taps, docs, resid, gain, ids, route,
    hid, tok, mixed, pad, dpad, mat, hc, hv, hd, wo, named, shares, table, turned_table,
    xbuf, pbuf, dbuf, r1, r2, rm, rz, rbz, rbp, acts, wg, wu, wd,
    in_sem, w_sem,
    s_a, r_a, s_b, s_h, r_h3, s_n, r_n, s_t, r_t,
    s_z, s_f, r_z, s_1, s_2, r_h, s_p, r_p,
    s_d, r_d, s_r1, r_r1, s_r2, r_r2, s_m, r_m, s_rz, r_rz,
    s_bz, r_bz, s_bp, r_bp, s_ap, r_ap, s_az, r_az, s_ao, r_ao,
):
    f32 = jnp.float32
    n_sp, n_tp = lax.axis_size("sp"), lax.axis_size("tp")
    nz = n_tp // 2
    width = out_ref.shape[1]
    half = width // 2
    rows = out_ref.shape[0]
    seq = gb.shape[0]
    halo = hc.shape[0]
    sp, tp = lax.axis_index("sp"), lax.axis_index("tp")
    y, x = sp // 2, sp % 2
    z, c = tp // 2, tp % 2
    xn, yn, dg = y * 2 + 1 - x, (1 - y) * 2 + x, (1 - y) * 2 + 1 - x
    columns = (sp, xn, yn, dg)
    OWN, XN, YN, DG = range(4)
    other = (sp, z * 2 + 1 - c)
    following, previous = (lax.rem(sp + 1, n_sp), tp), (lax.rem(sp + n_sp - 1, n_sp), tp)
    to_x, to_y = (xn, tp), (yn, tp)
    inner = z % 2 != z // 2
    outer = z % 2 == z // 2

    def zz(k):
        if k < 2:
            return 2 * (z // 2) + (z + k) % 2
        return k + (z // 2) * (nz - 1 - 2 * k)

    def slot(k, rel):
        return zz(k) * n_sp + columns[rel]

    def cols(h):
        return pl.ds(h * half, half)

    quarter = rbz.shape[3]
    share = (width - quarter) // 2

    def part(h):
        return pl.ds(h * share, share)

    body = pl.ds(0, 2 * share)
    along = pl.ds(2 * share, quarter)

    def rc(src, dst, ss, rs, dev):
        return pltpu.make_async_remote_copy(
            src_ref=src, dst_ref=dst, send_sem=ss, recv_sem=rs,
            device_id=dev, device_id_type=MESH,
        )


    def halo_copies():
        pairs = (
            (gc.at[pl.ds(seq - halo, halo)], hc),
            (vals.at[pl.ds(seq - halo, halo)], hv),
            (docs, hd),
        )
        return [rc(a, b, s_h.at[n], r_h3.at[n], following) for n, (a, b) in enumerate(pairs)]

    def channels(j):
        return pl.ds(pl.multiple_of(j * gb.shape[1], gb.shape[1]), gb.shape[1])

    def token_rows(j):
        return mixed.at[pl.ds(pl.multiple_of(j * rows, rows), rows)]

    def swap(d):
        j = lax.rem(tp + d, n_tp)
        return rc(token_rows(j), tok.at[:, channels(tp)], s_a.at[d], r_a.at[tp], (sp, j))

    def swapped(d):
        j = lax.rem(tp + d, n_tp)
        return rc(token_rows(j), tok.at[:, channels(j)], s_a.at[d], r_a.at[j], (sp, j))

    def swap_first():
        return rc(token_rows(0), tok.at[:, channels(tp)], s_b, r_a.at[tp], (sp, 0))


    def name_copy(rel):
        return rc(named.at[columns[rel]], shares.at[sp], s_n.at[rel], r_n.at[rel], (columns[rel], tp))

    def table_copy(d):
        return rc(shares, table.at[tp], s_t.at[d], r_t.at[tp], (sp, lax.rem(tp + d, n_tp)))

    def table_recv(d):
        j = lax.rem(tp + d, n_tp)
        return rc(shares, table.at[j], s_t.at[d], r_t.at[j], (sp, j))

    def name():
        named[...] = jnp.zeros_like(named)
        for e in range(n_sp):
            named[e, :, pl.ds(0, rows)] = jnp.where(ids[0:1] == e, route[0:1], 0.0) + jnp.where(
                ids[1:2] == e, route[1:2], 0.0
            )
        for rel in (XN, YN, DG):
            name_copy(rel).start()
        shares[sp] = named[sp]

    def tabulate():
        for d in range(1, n_tp):
            table_recv(d).wait_recv()
        mat[...] = jnp.zeros_like(mat)
        for j in range(n_tp):
            for e in range(n_sp):
                mat[pl.ds(j * n_sp + e, 1)] = table[j, e]
        turned_table[...] = mat[...].T

    def convolve(first, count):
        own = pl.ds(first, count)
        now = dpad[pl.ds(first + 8, count)]
        near = (dpad[pl.ds(first + 7, count)] == now).astype(f32)
        far = (dpad[pl.ds(first + 6, count)] == now).astype(f32)
        tap = taps[...].astype(f32)
        convolved = (
            tap[2:3] * pad[pl.ds(first + 8, count)]
            + tap[1:2] * pad[pl.ds(first + 7, count)] * near
            + tap[0:1] * pad[pl.ds(first + 6, count)] * far
        )
        mixed[own] = (gb[own].astype(f32) * convolved).astype(mixed.dtype)

    def mix():
        doc_rows = docs.shape[0]
        mat[...] = jnp.zeros_like(mat)
        mat[pl.ds(0, doc_rows)] = docs[...].astype(f32)
        turned = mat[...].T
        for n in range(doc_rows):
            dpad[pl.ds(8 + n * LANES, LANES)] = jnp.broadcast_to(
                turned[:, n : n + 1], (LANES, dpad.shape[1])
            )
        pad[pl.ds(8, seq)] = gc[...].astype(f32) * vals[...].astype(f32)
        pad[pl.ds(0, 8)] = jnp.zeros((8, pad.shape[1]), f32)
        dpad[pl.ds(0, 8)] = jnp.full((8, dpad.shape[1]), -1.0, f32)
        convolve(0, seq)
        for d in range(1, n_tp):
            @pl.when(lax.rem(tp + d, n_tp) != 0)
            def _():
                swap(d).start()

        mine = z * n_sp + sp

        for copy in halo_copies():
            copy.wait_recv()
        pad[pl.ds(0, 8)] = (hc[...].astype(f32) * hv[...].astype(f32))[halo - 8 :]
        last = hd[pl.ds(doc_rows - 1, 1)].astype(f32)
        last = jnp.where(sp == 0, -1.0, last)
        for n in (1, 2):
            dpad[pl.ds(8 - n, 1)] = jnp.broadcast_to(
                last[:, LANES - n : LANES - n + 1], (1, dpad.shape[1])
            )
        convolve(0, 16)

        @pl.when(tp != 0)
        def _():
            swap_first().start()

        for rel in (XN, YN, DG):
            name_copy(rel).wait_recv()
        table[tp] = shares[...]
        for d in range(1, n_tp):
            table_copy(d).start()

        tok[:, channels(tp)] = mixed[pl.ds(pl.multiple_of(tp * rows, rows), rows)]
        in_copies[5].wait()
        in_copies[6].wait()
        wo_copy.wait()
        for d in range(1, n_tp):
            swapped(d).wait_recv()
        projected = jnp.dot(tok[...], wo[...], preferred_element_type=f32)
        hidden = (resid[...].astype(f32) + projected).astype(hid.dtype)
        hid[...] = hidden
        state = hidden.astype(f32)
        scale = lax.rsqrt(jnp.mean(state * state, axis=-1, keepdims=True) + 1e-06)
        for n in range(width // LANES):
            at = slice(n * LANES, (n + 1) * LANES)
            xbuf[c, mine, :, pl.ds(n * LANES, LANES)] = (
                state[:, at] * scale * gain[n : n + 1].astype(f32)
            ).astype(xbuf.dtype)


    def z_send(k):
        at = xbuf.at[c, z * n_sp + sp, :, body]
        return rc(at, at, s_z.at[k], r_z.at[z], (sp, zz(k) * 2 + c))

    def z_recv(k):
        at = xbuf.at[c, slot(k, OWN), :, body]
        return rc(at, at, s_z.at[k], r_z.at[zz(k)], (sp, zz(k) * 2 + c))

    def forward(k):
        at = xbuf.at[c, slot(k, OWN), :, body]
        return rc(at, at, s_f.at[k], r_z.at[zz(k)], (sp, zz(2 if k == 1 else 1) * 2 + c))

    def pass_on(k):
        @pl.when(inner)
        def _():
            if k > 1:
                z_recv(k).wait_recv()
            forward(k).start()

    def piece(h, rel, k, ss, there, dev):
        at = xbuf.at[c, slot(k, rel), :, part(h)]
        return rc(at, at, ss, r_h.at[h, there, k], dev)

    def first(h, k):
        return piece(h, OWN, k, s_1.at[h, k], YN if h == 0 else XN, to_y if h == 0 else to_x)

    def second(h, k):
        return piece(h, OWN, k, s_2.at[h, 0, k], XN if h == 0 else YN, to_x if h == 0 else to_y)

    def third(h, k):
        return piece(h, YN if h == 0 else XN, k, s_2.at[h, 1, k], DG, to_x if h == 0 else to_y)

    def arrived(h, rel, k):
        piece(h, rel, k, s_1.at[h, k], rel, other).wait_recv()

    def to_other(rel, k):
        at = xbuf.at[c, slot(k, rel), :, body]
        return rc(at, at, s_p.at[k * n_sp + rel], r_p.at[k * n_sp + rel], other)


    def ap_copy(rel):
        at = xbuf.at[c, z * n_sp + sp, :, along]
        return rc(at, at, s_ap.at[rel], r_ap.at[rel], (columns[rel], tp))

    def ap_recv(rel):
        at = xbuf.at[c, slot(0, rel), :, along]
        return rc(at, at, s_ap.at[rel], r_ap.at[rel], (columns[rel], tp))

    def az_copy(k):
        at = xbuf.at[c, pl.ds(z * n_sp, n_sp), :, along]
        return rc(at, at, s_az.at[k], r_az.at[z], (sp, zz(k) * 2 + c))

    def az_recv(k):
        at = xbuf.at[c, group(k), :, along]
        return rc(at, at, s_az.at[k], r_az.at[zz(k)], (sp, zz(k) * 2 + c))

    def ao_copy(k):
        at = xbuf.at[c, group(k), :, along]
        return rc(at, at, s_ao.at[k], r_ao.at[k], other)

    def spread(k):
        for h in (1, 0):
            first(h, k).start()
        for h in (0, 1):
            second(h, k).start()
        to_other(OWN, k).start()

    def take(k):
        if k == 1:
            z_recv(k).wait_recv()
        else:
            @pl.when(outer)
            def _():
                z_recv(k).wait_recv()
        spread(k)

    def relay(k):
        arrived(0, YN, k)
        third(0, k).start()
        arrived(1, XN, k)
        third(1, k).start()

    def sides(k):
        if k > 0:
            az_recv(k).wait_recv()
            ao_copy(k).start()
        arrived(0, XN, k)
        to_other(XN, k).start()
        arrived(1, YN, k)
        to_other(YN, k).start()

    def corner(k):
        arrived(0, DG, k)
        arrived(1, DG, k)
        to_other(DG, k).start()


    def group(k):
        return pl.ds(zz(k) * n_sp, n_sp)

    def couple(at_z, s):
        row = y + s % 2 - 2 * y * (s % 2)
        return pl.ds(at_z * n_sp + 2 * row, 2)

    def d_copy(s):
        i = couple(zz(s // 2), s)
        return rc(pbuf.at[1 - c, i], dbuf.at[i], s_d.at[s], r_d.at[s], other)

    def merge(s):
        d_copy(s).wait_recv()
        i = couple(zz(s // 2), s)
        pbuf[c, i] = (pbuf[c, i].astype(f32) + dbuf[i].astype(f32)).astype(pbuf.dtype)

    def spread_along(k):
        bz_copy(k).start()

    def r1_copy(h, o, k):
        rel = DG if o else (XN if h == 0 else YN)
        at = pbuf.at[c, slot(k, rel), :, part(h)]
        return rc(at, r1.at[h, o, k], s_r1.at[h, o, k], r_r1.at[h, o, k], to_x if h == 0 else to_y)

    def r2_copy(h, k):
        at = pbuf.at[c, slot(k, YN if h == 0 else XN), :, part(h)]
        return rc(at, r2.at[h, k], s_r2.at[h, k], r_r2.at[h, k], to_y if h == 0 else to_x)

    def mate_copy(h, k):
        at = pbuf.at[c, slot(k, OWN), :, part(h)]
        return rc(at, rm.at[k - 2, :, part(h)], s_m.at[k - 2, h], r_m.at[k - 2, h], (sp, zz(1) * 2 + c))

    def rz_copy(h, k):
        n = min(k - 1, 1)
        at = pbuf.at[c, slot(k, OWN), :, part(h)]
        return rc(at, rz.at[n, :, part(h)], s_rz.at[k, h], r_rz.at[n, h], (sp, zz(k) * 2 + c))

    def bz_copy(k):
        return rc(
            pbuf.at[c, group(k), :, along], rbz.at[z], s_bz.at[k], r_bz.at[z], (sp, zz(k) * 2 + c)
        )

    def bz_recv(k):
        return rc(
            pbuf.at[c, group(k), :, along], rbz.at[zz(k)], s_bz.at[k], r_bz.at[zz(k)],
            (sp, zz(k) * 2 + c),
        )

    def bp_copy(rel):
        return rc(
            pbuf.at[c, slot(0, rel), :, along], rbp.at[rel], s_bp.at[rel], r_bp.at[rel],
            (columns[rel], tp),
        )

    def along_sum():
        total = pbuf[c, group(0), :, along].astype(f32)
        for k in range(1, nz):
            bz_recv(k).wait_recv()
            total = total + rbz[zz(k)].astype(f32)
        pbuf[c, group(0), :, along] = total.astype(pbuf.dtype)
        for rel in (DG, XN, YN):
            bp_copy(rel).start()

    def stage1(k, parts=(1, 0)):
        for o in parts:
            for h in (0, 1):
                r1_copy(h, o, k).start()

    def stage2(k):
        for h in (0, 1):
            r1_copy(h, 1, k).wait_recv()
            i = slot(k, YN if h == 0 else XN)
            pbuf[c, i, :, part(h)] = (
                pbuf[c, i, :, part(h)].astype(f32) + r1[h, 1, k].astype(f32)
            ).astype(pbuf.dtype)
            r2_copy(h, k).start()

    def summed(h, k):
        r1_copy(h, 0, k).wait_recv()
        r2_copy(h, k).wait_recv()
        return (
            pbuf[c, slot(k, OWN), :, part(h)].astype(f32)
            + r1[h, 0, k].astype(f32)
            + r2[h, k].astype(f32)
        )

    def stage3(k):
        for h in (0, 1):
            pbuf[c, slot(k, OWN), :, part(h)] = summed(h, k).astype(pbuf.dtype)
            if k == 1:
                rz_copy(h, k).start()
            else:
                @pl.when(outer)
                def _():
                    mate_copy(h, k).start()

    def stage4(k):
        @pl.when(inner)
        def _():
            at = slot(k, OWN)
            for h in (0, 1):
                mate_copy(h, k).wait_recv()
                pbuf[c, at, :, part(h)] = (
                    pbuf[c, at, :, part(h)].astype(f32) + rm[k - 2, :, part(h)].astype(f32)
                ).astype(pbuf.dtype)
                rz_copy(h, k).start()

    barrier = pltpu.get_barrier_semaphore()
    peers = [to_x, to_y, (dg, tp), following, previous] + [(sp, lax.rem(tp + d, n_tp)) for d in range(1, n_tp)]
    for peer in peers:
        pl.semaphore_signal(barrier, inc=1, device_id=peer, device_id_type=MESH)
    in_copies = [
        pltpu.make_async_copy(a, b, in_sem.at[n])
        for n, (a, b) in enumerate((
            (gc_hbm, gc), (vals_hbm, vals), (docs_hbm, docs), (taps_hbm, taps), (gb_hbm, gb),
            (resid_hbm, resid), (gain_hbm, gain), (ids_hbm, ids), (route_hbm, route),
        ))
    ]
    weights = [
        pltpu.make_async_copy(a, b, w_sem.at[n])
        for n, (a, b) in enumerate(((wg_hbm, wg), (wu_hbm, wu), (wd_hbm, wd)))
    ]
    wo_copy = pltpu.make_async_copy(wo_hbm, wo, w_sem.at[3])
    for copy in in_copies:
        copy.start()
    wo_copy.start()
    for w in weights:
        w.start()
    for n in (0, 1, 2):
        in_copies[n].wait()
    pl.semaphore_wait(barrier, len(peers))
    for copy in halo_copies():
        copy.start()
    for n in (3, 4, 7, 8):
        in_copies[n].wait()
    name()
    mix()
    for rel in (DG, XN, YN):
        ap_copy(rel).start()
    for h in (1, 0):
        first(h, 0).start()
    z_send(1).start()

    @pl.when(inner)
    def _():
        z_send(2).start()

    for h in (0, 1):
        second(h, 0).start()
    to_other(OWN, 0).start()
    for rel in (XN, YN, DG):
        ap_recv(rel).wait_recv()
    az_copy(1).start()
    ao_copy(0).start()
    relay(0)
    take(1)
    pass_on(1)
    pass_on(2)
    az_copy(2).start()
    az_copy(3).start()
    sides(0)
    tabulate()
    for w in weights:
        w.wait()

    lane = lax.broadcasted_iota(jnp.int32, (rows, LANES), 1)
    steps = 2 * nz
    before, middle, after = {}, {}, {}

    def put(table, s, work, *args):
        table.setdefault(s, []).append(functools.partial(work, *args))

    end = nz - 1
    put(before, 1, relay, 1)
    put(middle, 0, corner, 0)
    put(middle, 1, pass_on, end)
    for k in range(1, nz):
        if k < end:
            put(middle, 2 * k - 1, take, k + 1)
            put(middle, 2 * k, relay, k + 1)
        else:
            put(middle, 2 * k, stage2, 1)
        put(middle, 2 * k - 1, sides, k)
        put(middle, 2 * k, corner, k)
    for s in range(1, 2 * end):
        put(after, s, merge, s - 1)
    for k in range(1, end - 1):
        put(after, 2 * k + 2, spread_along, k)
    put(before, 2 * end - 1, stage1, 1)
    put(middle, 2 * end, merge, 2 * end - 1)
    put(middle, 2 * end, stage1, end - 1)
    put(middle, 2 * end, spread_along, end - 1)
    put(middle, 2 * end + 1, merge, 2 * end)

    @pl.loop(0, steps)
    def _(s):
        for at, works in before.items():
            @pl.when(s == at)
            def _():
                for work in works:
                    work()

        k = s // 2
        side = s % 2
        at_z = jnp.where(k < 2, 2 * (z // 2) + (z + k) % 2, k + (z // 2) * (nz - 1 - 2 * k))
        for b in (0, 1):
            column = jnp.where(side == 0, columns[b], columns[2 + b])
            at = xbuf.at[1 - c, at_z * n_sp + column, :, body]
            n = k * n_sp + 2 * side + b
            rc(at, at, s_p.at[n], r_p.at[n], other).wait_recv()

        @pl.when(side == 0)
        def _():
            at = xbuf.at[1 - c, pl.ds(at_z * n_sp, n_sp), :, along]
            rc(at, at, s_ao.at[k], r_ao.at[k], other).wait_recv()

        i = couple(at_z, s)
        held = xbuf[:, i].reshape(4 * rows, width)
        row = y + side - 2 * y * side
        scale = jnp.concatenate(
            [
                jnp.sum(
                    jnp.where(
                        lane == (at_z * 2 + core) * n_sp + 2 * row + e,
                        turned_table[pl.ds(0, rows)], 0.0,
                    ),
                    axis=1,
                    keepdims=True,
                )
                for core in (0, 1)
                for e in (0, 1)
            ],
            axis=0,
        )
        gate = jnp.dot(held, wg[...], preferred_element_type=f32)
        up = jnp.dot(held, wu[...], preferred_element_type=f32)
        acts[...] = (jax.nn.silu(gate) * up * scale).astype(acts.dtype)

        for at, works in middle.items():
            @pl.when(s == at)
            def _():
                for work in works:
                    work()

        down = jnp.dot(acts[...], wd[...], preferred_element_type=f32)
        pbuf[:, i] = down.astype(pbuf.dtype).reshape(2, 2, rows, width)
        rc(pbuf.at[1 - c, i], dbuf.at[i], s_d.at[s], r_d.at[s], other).start()

        for at, works in after.items():
            @pl.when(s == at)
            def _():
                for work in works:
                    work()

    stage3(1)
    stage2(end - 1)
    merge(2 * end + 1)
    stage1(end)
    stage3(end - 1)
    spread_along(end)
    stage2(end)
    stage1(0)
    stage4(end - 1)
    stage3(end)
    stage2(0)
    along_sum()
    stage4(end)
    for h in (0, 1):
        total = hid[:, part(h)].astype(f32) + summed(h, 0)
        for n in (0, 1):
            rz_copy(h, n + 1).wait_recv()
            total = total + rz[n, :, part(h)].astype(f32)
        out_ref[:, part(h)] = total.astype(out_ref.dtype)
    total = hid[:, along].astype(f32) + pbuf[c, slot(0, OWN), :, along].astype(f32)
    for rel in (XN, YN, DG):
        bp_copy(rel).wait_recv()
        total = total + rbp[rel].astype(f32)
    out_ref[:, along] = total.astype(out_ref.dtype)

    for copy in halo_copies():
        copy.wait_send()
    for d in range(1, n_tp):
        @pl.when(lax.rem(tp + d, n_tp) != 0)
        def _():
            swap(d).wait_send()

    @pl.when(tp != 0)
    def _():
        swap_first().wait_send()

    for rel in (XN, YN, DG):
        name_copy(rel).wait_send()
        bp_copy(rel).wait_send()
        ap_copy(rel).wait_send()
    for k in range(1, nz):
        bz_copy(k).wait_send()
        az_copy(k).wait_send()
    for k in range(nz):
        ao_copy(k).wait_send()
    for d in range(1, n_tp):
        table_copy(d).wait_send()
    z_send(1).wait_send()
    for h in (0, 1):
        rz_copy(h, 1).wait_send()

    @pl.when(inner)
    def _():
        z_send(2).wait_send()
        for k in range(1, nz):
            forward(k).wait_send()
        for k in range(2, nz):
            for h in (0, 1):
                rz_copy(h, k).wait_send()

    @pl.when(outer)
    def _():
        for k in range(2, nz):
            for h in (0, 1):
                mate_copy(h, k).wait_send()

    for k in range(nz):
        for h in (0, 1):
            first(h, k).wait_send()
            second(h, k).wait_send()
            third(h, k).wait_send()
            r1_copy(h, 0, k).wait_send()
            r1_copy(h, 1, k).wait_send()
            r2_copy(h, k).wait_send()
        for rel in range(n_sp):
            to_other(rel, k).wait_send()
    for s in range(steps):
        d_copy(s).wait_send()


def layer(gate_b, gate_c, values_in, conv_w, docs, resid, gain, ids, route, w_out, w_gate, w_up, w_down):
    rows, width = resid.shape
    seq, held = gate_b.shape
    n_tp = lax.axis_size("tp")
    n_sp = lax.axis_size("sp")
    nz = n_tp // 2
    quarter = width // 8
    share = (width - quarter) // 2
    bf = jnp.bfloat16
    f32 = jnp.float32
    dma = pltpu.SemaphoreType.DMA
    hbm = pl.BlockSpec(memory_space=pl.ANY)
    vmem = pl.BlockSpec(memory_space=pltpu.VMEM)
    operands = (gate_b, gate_c, values_in, conv_w, docs, resid, gain, ids, route)
    return pl.pallas_call(
        moe_kernel,
        out_shape=pltpu.VMEM((rows, width), bf),
        in_specs=[hbm] * 13,
        out_specs=vmem,
        scratch_shapes=[pltpu.VMEM(a.shape, a.dtype) for a in operands] + [
            pltpu.VMEM((rows, width), bf),
            pltpu.VMEM((rows, n_tp * held), bf),
            pltpu.VMEM((seq, held), bf),
            pltpu.VMEM((seq + 8, held), f32),
            pltpu.VMEM((seq + 8, held), f32),
            pltpu.VMEM((LANES, LANES), f32),
            pltpu.VMEM((16, held), bf),
            pltpu.VMEM((16, held), bf),
            pltpu.VMEM(docs.shape, docs.dtype),
            pltpu.VMEM(w_out.shape, bf),
            pltpu.VMEM((n_sp, 1, LANES), f32),
            pltpu.VMEM((n_sp, 1, LANES), f32),
            pltpu.VMEM((n_tp, n_sp, 1, LANES), f32),
            pltpu.VMEM((LANES, LANES), f32),
            pltpu.VMEM((2, n_sp * nz, rows, width), bf),
            pltpu.VMEM((2, n_sp * nz, rows, width), bf),
            pltpu.VMEM((n_sp * nz, rows, width), bf),
            pltpu.VMEM((2, 2, nz, rows, share), bf),
            pltpu.VMEM((2, nz, rows, share), bf),
            pltpu.VMEM((2, rows, 2 * share), bf),
            pltpu.VMEM((2, rows, 2 * share), bf),
            pltpu.VMEM((nz, n_sp, rows, quarter), bf),
            pltpu.VMEM((4, rows, quarter), bf),
            pltpu.VMEM((4 * rows, w_gate.shape[1]), bf),
            pltpu.VMEM(w_gate.shape, bf),
            pltpu.VMEM(w_up.shape, bf),
            pltpu.VMEM(w_down.shape, bf),
            dma((9,)), dma((4,)),
            dma((n_tp,)), dma((n_tp,)), dma, dma((3,)), dma((3,)),
            dma((4,)), dma((4,)), dma((n_tp,)), dma((n_tp,)),
            dma((nz,)), dma((nz,)), dma((nz,)), dma((2, nz)), dma((2, 2, nz)), dma((2, 4, nz)),
            dma((n_sp * nz,)), dma((n_sp * nz,)),
            dma((2 * nz,)), dma((2 * nz,)),
            dma((2, 2, nz)), dma((2, 2, nz)), dma((2, nz)), dma((2, nz)),
            dma((2, 2)), dma((2, 2)), dma((nz, 2)), dma((2, 2)),
            dma((nz,)), dma((nz,)), dma((4,)), dma((4,)),
            dma((4,)), dma((4,)), dma((nz,)), dma((nz,)), dma((nz,)), dma((nz,)),
        ],
        compiler_params=pltpu.CompilerParams(
            collective_id=0, has_side_effects=True, vmem_limit_bytes=64000000
        ),
    )(*operands, w_out, w_gate, w_up, w_down)


def passed_along(block, axis, distance):
    devices = range(lax.axis_size(axis))
    route = [(i - distance, i) for i in devices if i - distance in devices]
    return lax.ppermute(block, axis, route)


def local(
    gate_b,
    gate_c,
    values_in,
    conv_w,
    documents,
    w_out,
    resid,
    norm_gain,
    route_ids,
    route_weight,
    w_gate,
    w_up,
    w_down,
):
    seq_rows = gate_b.shape[0]
    local_rows = resid.shape[0]
    model_width = resid.shape[1]
    experts = lax.axis_size("sp") * w_gate.shape[0]
    capacity = 4 * local_rows // experts
    if (lax.axis_size("sp"), lax.axis_size("tp")) == (4, 8) and w_gate.shape[0] == 1 and capacity >= local_rows:
        return layer(
            gate_b, gate_c, values_in, conv_w, documents.reshape(-1, LANES), resid,
            norm_gain.reshape(-1, LANES), route_ids.T, route_weight.T,
            w_out, w_gate[0], w_up[0], w_down[0],
        )
    last_rows = jnp.stack([gate_c[seq_rows - 2 :], values_in[seq_rows - 2 :]])
    before, before_docs = passed_along((last_rows, documents[seq_rows - 2 :]), "sp", 1)
    products = jnp.concatenate(
        [
            before[0].astype(jnp.float32) * before[1].astype(jnp.float32),
            gate_c.astype(jnp.float32) * values_in.astype(jnp.float32),
        ],
        axis=0,
    )
    docs_all = jnp.concatenate([before_docs, documents], axis=0)
    kernel_taps = conv_w.astype(jnp.float32)
    near_mask = (docs_all[1:-1] == documents).astype(jnp.float32)[:, None]
    far_mask = (docs_all[:-2] == documents).astype(jnp.float32)[:, None]
    convolved = (
        kernel_taps[2] * products[2:]
        + kernel_taps[1] * products[1:-1] * near_mask
        + kernel_taps[0] * products[:-2] * far_mask
    )
    mixed_rows = (gate_b.astype(jnp.float32) * convolved).astype(jnp.bfloat16)
    token_rows = lax.all_to_all(mixed_rows, "tp", split_axis=0, concat_axis=1, tiled=True)
    projected = jnp.dot(token_rows, w_out, preferred_element_type=jnp.float32)
    hidden_state = (resid.astype(jnp.float32) + projected).astype(jnp.bfloat16)
    state_wide = hidden_state.astype(jnp.float32)
    normed = (
        state_wide
        * lax.rsqrt(jnp.mean(state_wide * state_wide, axis=-1, keepdims=True) + 1e-06)
        * norm_gain.astype(jnp.float32)
    ).astype(jnp.bfloat16)
    experts = lax.axis_size("sp") * w_gate.shape[0]
    capacity = 4 * local_rows // experts
    flat_ids = route_ids.reshape(-1)
    one_hot = (flat_ids[:, None] == jnp.arange(experts, dtype=jnp.int32)[None, :]).astype(jnp.int32)
    rank_in = jnp.sum((jnp.cumsum(one_hot, axis=0) - one_hot) * one_hot, axis=1)
    slot_index = flat_ids * capacity + rank_in
    placement = (
        slot_index[:, None] == jnp.arange(experts * capacity, dtype=jnp.int32)[None, :]
    ).astype(jnp.bfloat16)
    repeated = jnp.repeat(normed, 2, axis=0)
    dispatch = jnp.einsum(
        "js,jd->sd", placement, repeated, preferred_element_type=jnp.float32
    ).astype(jnp.bfloat16)
    dispatch = dispatch.reshape(experts, capacity, model_width)
    gathered_piece = lax.all_gather(
        lax.all_to_all(dispatch, "sp", split_axis=0, concat_axis=0, tiled=True),
        "tp",
        axis=0,
        tiled=True,
    )
    flat_rows = gathered_piece.reshape(-1, model_width)
    gate_part = jnp.dot(flat_rows, w_gate[0], preferred_element_type=jnp.float32)
    up_part = jnp.dot(flat_rows, w_up[0], preferred_element_type=jnp.float32)
    activated = (jax.nn.silu(gate_part) * up_part).astype(jnp.bfloat16)
    partial_value = jnp.dot(activated, w_down[0], preferred_element_type=jnp.float32)
    partial_value = partial_value.reshape(
        gathered_piece.shape[0], gathered_piece.shape[1], model_width
    )
    summed = lax.psum_scatter(
        partial_value.astype(jnp.bfloat16), "tp", scatter_dimension=0, tiled=True
    )
    returned = lax.all_to_all(summed, "sp", split_axis=0, concat_axis=0, tiled=True)
    picked = jnp.take(
        returned.reshape(experts * capacity, model_width), slot_index, axis=0
    ).reshape(local_rows, 2, model_width)
    combined = jnp.sum(route_weight[:, :, None] * picked.astype(jnp.float32), axis=1)
    return (hidden_state.astype(jnp.float32) + combined).astype(jnp.bfloat16)


def solution(mesh):
    return jax.shard_map(
        local,
        mesh=mesh,
        in_specs=(
            P("sp", "tp"),
            P("sp", "tp"),
            P("sp", "tp"),
            P(None, "tp"),
            P("sp"),
            P(),
            P(("sp", "tp"), None),
            P(),
            P(("sp", "tp"), None),
            P(("sp", "tp"), None),
            P("sp", None, "tp"),
            P("sp", None, "tp"),
            P("sp", "tp", None),
        ),
        out_specs=P(("sp", "tp"), None),
        check_vma=False,
    )
```

```python
import functools

import jax
import jax.numpy as jnp
from jax import lax
from jax.experimental import pallas as pl
from jax.experimental.pallas import tpu as pltpu
from jax.sharding import PartitionSpec as P

MESH = pl.DeviceIdType.MESH
LANES = 128


def moe_kernel(
    gb_hbm, gc_hbm, vals_hbm, taps_hbm, docs_hbm, resid_hbm, gain_hbm, ids_hbm, route_hbm,
    wo_hbm, wg_hbm, wu_hbm, wd_hbm, out_ref,
    gb, gc, vals, taps, docs, resid, gain, ids, route,
    hid, tok, mixed, pad, dpad, mat, hc, hv, hd, wo, named, shares, table, turned_table,
    xbuf, pbuf, dbuf, r1, r2, rm, rz, rbz, rbp, acts, wg, wu, wd,
    in_sem, w_sem,
    s_a, r_a, s_h, r_h3, s_n, r_n, s_t, r_t,
    s_z, s_f, r_z, s_1, s_2, r_h, s_p, r_p,
    s_d, r_d, s_r1, r_r1, s_r2, r_r2, s_m, r_m, s_rz, r_rz,
    s_bz, r_bz, s_bp, r_bp, s_ap, r_ap, s_az, r_az, s_ao, r_ao,
):
    f32 = jnp.float32
    n_sp, n_tp = lax.axis_size("sp"), lax.axis_size("tp")
    nz = n_tp // 2
    width = out_ref.shape[1]
    half = width // 2
    rows = out_ref.shape[0]
    seq = gb.shape[0]
    halo = hc.shape[0]
    sp, tp = lax.axis_index("sp"), lax.axis_index("tp")
    y, x = sp // 2, sp % 2
    z, c = tp // 2, tp % 2
    xn, yn, dg = y * 2 + 1 - x, (1 - y) * 2 + x, (1 - y) * 2 + 1 - x
    columns = (sp, xn, yn, dg)
    OWN, XN, YN, DG = range(4)
    other = (sp, z * 2 + 1 - c)
    following, previous = (lax.rem(sp + 1, n_sp), tp), (lax.rem(sp + n_sp - 1, n_sp), tp)
    to_x, to_y = (xn, tp), (yn, tp)
    inner = z % 2 != z // 2
    outer = z % 2 == z // 2

    def zz(k):
        if k < 2:
            return 2 * (z // 2) + (z + k) % 2
        return k + (z // 2) * (nz - 1 - 2 * k)

    def slot(k, rel):
        return zz(k) * n_sp + columns[rel]

    def cols(h):
        return pl.ds(h * half, half)

    quarter = rbz.shape[3]
    share = (width - quarter) // 2

    def part(h):
        return pl.ds(h * share, share)

    body = pl.ds(0, 2 * share)
    along = pl.ds(2 * share, quarter)

    def rc(src, dst, ss, rs, dev):
        return pltpu.make_async_remote_copy(
            src_ref=src, dst_ref=dst, send_sem=ss, recv_sem=rs,
            device_id=dev, device_id_type=MESH,
        )


    def halo_copies():
        pairs = (
            (gc.at[pl.ds(seq - halo, halo)], hc),
            (vals.at[pl.ds(seq - halo, halo)], hv),
            (docs, hd),
        )
        return [rc(a, b, s_h.at[n], r_h3.at[n], following) for n, (a, b) in enumerate(pairs)]

    def channels(j):
        return pl.ds(pl.multiple_of(j * gb.shape[1], gb.shape[1]), gb.shape[1])

    def token_rows(j):
        return mixed.at[pl.ds(pl.multiple_of(j * rows, rows), rows)]

    def swap(d):
        j = lax.rem(tp + d, n_tp)
        return rc(token_rows(j), tok.at[:, channels(tp)], s_a, r_a, (sp, j))

    def swaps():
        at = tok.at[:, pl.ds(0, (n_tp - 1) * gb.shape[1])]
        return rc(at, at, s_a, r_a, other)

    def swap_first():
        return rc(token_rows(0), tok.at[:, channels(tp)], s_a, r_a, (sp, 0))


    def name_copy(rel):
        return rc(named.at[columns[rel]], shares.at[sp], s_n, r_n.at[rel], (columns[rel], tp))

    def table_copy(d):
        return rc(shares, table.at[tp], s_t, r_t, (sp, lax.rem(tp + d, n_tp)))

    def tables():
        at = table.at[pl.ds(0, n_tp - 1)]
        return rc(at, at, s_t, r_t, other)

    def name():
        named[...] = jnp.zeros_like(named)
        for e in range(n_sp):
            named[e, :, pl.ds(0, rows)] = jnp.where(ids[0:1] == e, route[0:1], 0.0) + jnp.where(
                ids[1:2] == e, route[1:2], 0.0
            )
        for rel in (XN, YN, DG):
            name_copy(rel).start()
        shares[sp] = named[sp]

    def tabulate():
        tables().wait_recv()
        mat[...] = jnp.zeros_like(mat)
        for j in range(n_tp):
            for e in range(n_sp):
                mat[pl.ds(j * n_sp + e, 1)] = table[j, e]
        turned_table[...] = mat[...].T

    def convolve(first, count):
        own = pl.ds(first, count)
        now = dpad[pl.ds(first + 8, count)]
        near = (dpad[pl.ds(first + 7, count)] == now).astype(f32)
        far = (dpad[pl.ds(first + 6, count)] == now).astype(f32)
        tap = taps[...].astype(f32)
        convolved = (
            tap[2:3] * pad[pl.ds(first + 8, count)]
            + tap[1:2] * pad[pl.ds(first + 7, count)] * near
            + tap[0:1] * pad[pl.ds(first + 6, count)] * far
        )
        mixed[own] = (gb[own].astype(f32) * convolved).astype(mixed.dtype)

    def mix():
        doc_rows = docs.shape[0]
        mat[...] = jnp.zeros_like(mat)
        mat[pl.ds(0, doc_rows)] = docs[...].astype(f32)
        turned = mat[...].T
        for n in range(doc_rows):
            dpad[pl.ds(8 + n * LANES, LANES)] = jnp.broadcast_to(
                turned[:, n : n + 1], (LANES, dpad.shape[1])
            )
        pad[pl.ds(8, seq)] = gc[...].astype(f32) * vals[...].astype(f32)
        pad[pl.ds(0, 8)] = jnp.zeros((8, pad.shape[1]), f32)
        dpad[pl.ds(0, 8)] = jnp.full((8, dpad.shape[1]), -1.0, f32)
        convolve(0, seq)
        for d in range(1, n_tp):
            @pl.when(lax.rem(tp + d, n_tp) != 0)
            def _():
                swap(d).start()

        mine = z * n_sp + sp

        for copy in halo_copies():
            copy.wait_recv()
        pad[pl.ds(0, 8)] = (hc[...].astype(f32) * hv[...].astype(f32))[halo - 8 :]
        last = hd[pl.ds(doc_rows - 1, 1)].astype(f32)
        last = jnp.where(sp == 0, -1.0, last)
        for n in (1, 2):
            dpad[pl.ds(8 - n, 1)] = jnp.broadcast_to(
                last[:, LANES - n : LANES - n + 1], (1, dpad.shape[1])
            )
        convolve(0, 16)

        @pl.when(tp != 0)
        def _():
            swap_first().start()

        for rel in (XN, YN, DG):
            name_copy(rel).wait_recv()
        table[tp] = shares[...]
        for d in range(1, n_tp):
            table_copy(d).start()

        tok[:, channels(tp)] = mixed[pl.ds(pl.multiple_of(tp * rows, rows), rows)]
        in_copies[5].wait()
        in_copies[6].wait()
        wo_copy.wait()
        swaps().wait_recv()
        projected = jnp.dot(tok[...], wo[...], preferred_element_type=f32)
        hidden = (resid[...].astype(f32) + projected).astype(hid.dtype)
        hid[...] = hidden
        state = hidden.astype(f32)
        scale = lax.rsqrt(jnp.mean(state * state, axis=-1, keepdims=True) + 1e-06)
        for n in range(width // LANES):
            at = slice(n * LANES, (n + 1) * LANES)
            xbuf[c, mine, :, pl.ds(n * LANES, LANES)] = (
                state[:, at] * scale * gain[n : n + 1].astype(f32)
            ).astype(xbuf.dtype)


    def z_send(k):
        at = xbuf.at[c, z * n_sp + sp, :, body]
        return rc(at, at, s_z.at[k], r_z.at[z], (sp, zz(k) * 2 + c))

    def z_recv(k):
        at = xbuf.at[c, slot(k, OWN), :, body]
        return rc(at, at, s_z.at[k], r_z.at[zz(k)], (sp, zz(k) * 2 + c))

    def forward(k):
        at = xbuf.at[c, slot(k, OWN), :, body]
        return rc(at, at, s_f.at[k], r_z.at[zz(k)], (sp, zz(2 if k == 1 else 1) * 2 + c))

    def pass_on(k):
        @pl.when(inner)
        def _():
            if k > 1:
                z_recv(k).wait_recv()
            forward(k).start()

    def piece(h, rel, k, ss, there, dev):
        at = xbuf.at[c, slot(k, rel), :, part(h)]
        return rc(at, at, ss, r_h.at[h, there, k], dev)

    def first(h, k):
        return piece(h, OWN, k, s_1, YN if h == 0 else XN, to_y if h == 0 else to_x)

    def second(h, k):
        return piece(h, OWN, k, s_2, XN if h == 0 else YN, to_x if h == 0 else to_y)

    def third(h, k):
        return piece(h, YN if h == 0 else XN, k, s_2, DG, to_x if h == 0 else to_y)

    def arrived(h, rel, k):
        piece(h, rel, k, s_1, rel, other).wait_recv()

    def to_other(rel, k):
        at = xbuf.at[c, slot(k, rel), :, body]
        return rc(at, at, s_p, r_p.at[k * n_sp + rel], other)


    def ap_copy(rel):
        at = xbuf.at[c, z * n_sp + sp, :, along]
        return rc(at, at, s_ap, r_ap.at[rel], (columns[rel], tp))

    def ap_recv(rel):
        at = xbuf.at[c, slot(0, rel), :, along]
        return rc(at, at, s_ap, r_ap.at[rel], (columns[rel], tp))

    def az_copy(k):
        at = xbuf.at[c, pl.ds(z * n_sp, n_sp), :, along]
        return rc(at, at, s_az, r_az.at[z], (sp, zz(k) * 2 + c))

    def az_recv(k):
        at = xbuf.at[c, group(k), :, along]
        return rc(at, at, s_az, r_az.at[zz(k)], (sp, zz(k) * 2 + c))

    def ao_copy(k):
        at = xbuf.at[c, group(k), :, along]
        return rc(at, at, s_ao, r_ao.at[k], other)

    def spread(k):
        for h in (1, 0):
            first(h, k).start()
        for h in (0, 1):
            second(h, k).start()
        to_other(OWN, k).start()

    def take(k):
        if k == 1:
            z_recv(k).wait_recv()
        else:
            @pl.when(outer)
            def _():
                z_recv(k).wait_recv()
        spread(k)

    def relay(k):
        arrived(0, YN, k)
        third(0, k).start()
        arrived(1, XN, k)
        third(1, k).start()

    def sides(k):
        if k > 0:
            az_recv(k).wait_recv()
            ao_copy(k).start()
        arrived(0, XN, k)
        to_other(XN, k).start()
        arrived(1, YN, k)
        to_other(YN, k).start()

    def corner(k):
        arrived(0, DG, k)
        arrived(1, DG, k)
        to_other(DG, k).start()


    def group(k):
        return pl.ds(zz(k) * n_sp, n_sp)

    def couple(at_z, s):
        row = y + s % 2 - 2 * y * (s % 2)
        return pl.ds(at_z * n_sp + 2 * row, 2)

    def d_copy(s):
        i = couple(zz(s // 2), s)
        return rc(pbuf.at[1 - c, i], dbuf.at[i], s_d, r_d.at[s], other)

    def merge(s):
        d_copy(s).wait_recv()
        i = couple(zz(s // 2), s)
        pbuf[c, i] = (pbuf[c, i].astype(f32) + dbuf[i].astype(f32)).astype(pbuf.dtype)

    def spread_along(k):
        bz_copy(k).start()

    def r1_copy(h, o, k):
        rel = DG if o else (XN if h == 0 else YN)
        at = pbuf.at[c, slot(k, rel), :, part(h)]
        return rc(at, r1.at[h, o, k], s_r1, r_r1.at[h, o, k], to_x if h == 0 else to_y)

    def r2_copy(h, k):
        at = pbuf.at[c, slot(k, YN if h == 0 else XN), :, part(h)]
        return rc(at, r2.at[h, k], s_r2, r_r2.at[h, k], to_y if h == 0 else to_x)

    def mate_copy(h, k):
        at = pbuf.at[c, slot(k, OWN), :, part(h)]
        return rc(at, rm.at[k - 2, :, part(h)], s_m.at[k - 2, h], r_m.at[k - 2, h], (sp, zz(1) * 2 + c))

    def rz_copy(h, k):
        n = min(k - 1, 1)
        at = pbuf.at[c, slot(k, OWN), :, part(h)]
        return rc(at, rz.at[n, :, part(h)], s_rz.at[k, h], r_rz.at[n, h], (sp, zz(k) * 2 + c))

    def bz_copy(k):
        return rc(
            pbuf.at[c, group(k), :, along], rbz.at[z], s_bz, r_bz.at[z], (sp, zz(k) * 2 + c)
        )

    def bz_recv(k):
        return rc(
            pbuf.at[c, group(k), :, along], rbz.at[zz(k)], s_bz, r_bz.at[zz(k)],
            (sp, zz(k) * 2 + c),
        )

    def bp_copy(rel):
        return rc(
            pbuf.at[c, slot(0, rel), :, along], rbp.at[rel], s_bp, r_bp.at[rel],
            (columns[rel], tp),
        )

    def along_sum():
        total = pbuf[c, group(0), :, along].astype(f32)
        for k in range(1, nz):
            bz_recv(k).wait_recv()
            total = total + rbz[zz(k)].astype(f32)
        pbuf[c, group(0), :, along] = total.astype(pbuf.dtype)
        for rel in (DG, XN, YN):
            bp_copy(rel).start()

    def stage1(k, parts=(1, 0)):
        for o in parts:
            for h in (0, 1):
                r1_copy(h, o, k).start()

    def stage2(k):
        for h in (0, 1):
            r1_copy(h, 1, k).wait_recv()
            i = slot(k, YN if h == 0 else XN)
            pbuf[c, i, :, part(h)] = (
                pbuf[c, i, :, part(h)].astype(f32) + r1[h, 1, k].astype(f32)
            ).astype(pbuf.dtype)
            r2_copy(h, k).start()

    def summed(h, k):
        r1_copy(h, 0, k).wait_recv()
        r2_copy(h, k).wait_recv()
        return (
            pbuf[c, slot(k, OWN), :, part(h)].astype(f32)
            + r1[h, 0, k].astype(f32)
            + r2[h, k].astype(f32)
        )

    def stage3(k):
        for h in (0, 1):
            pbuf[c, slot(k, OWN), :, part(h)] = summed(h, k).astype(pbuf.dtype)
            if k == 1:
                rz_copy(h, k).start()
            else:
                @pl.when(outer)
                def _():
                    mate_copy(h, k).start()

    def stage4(k):
        @pl.when(inner)
        def _():
            at = slot(k, OWN)
            for h in (0, 1):
                mate_copy(h, k).wait_recv()
                pbuf[c, at, :, part(h)] = (
                    pbuf[c, at, :, part(h)].astype(f32) + rm[k - 2, :, part(h)].astype(f32)
                ).astype(pbuf.dtype)
                rz_copy(h, k).start()

    barrier = pltpu.get_barrier_semaphore()
    peers = [to_x, to_y, (dg, tp), following, previous] + [(sp, lax.rem(tp + d, n_tp)) for d in range(1, n_tp)]
    for peer in peers:
        pl.semaphore_signal(barrier, inc=1, device_id=peer, device_id_type=MESH)
    in_copies = [
        pltpu.make_async_copy(a, b, in_sem.at[n])
        for n, (a, b) in enumerate((
            (gc_hbm, gc), (vals_hbm, vals), (docs_hbm, docs), (taps_hbm, taps), (gb_hbm, gb),
            (resid_hbm, resid), (gain_hbm, gain), (ids_hbm, ids), (route_hbm, route),
        ))
    ]
    weights = [
        pltpu.make_async_copy(a, b, w_sem.at[n])
        for n, (a, b) in enumerate(((wg_hbm, wg), (wu_hbm, wu), (wd_hbm, wd)))
    ]
    wo_copy = pltpu.make_async_copy(wo_hbm, wo, w_sem.at[3])
    for copy in in_copies:
        copy.start()
    wo_copy.start()
    for w in weights:
        w.start()
    for n in (0, 1, 2):
        in_copies[n].wait()
    pl.semaphore_wait(barrier, len(peers))
    for copy in halo_copies():
        copy.start()
    for n in (3, 4, 7, 8):
        in_copies[n].wait()
    name()
    mix()
    for rel in (DG, XN, YN):
        ap_copy(rel).start()
    for h in (1, 0):
        first(h, 0).start()
    z_send(1).start()

    @pl.when(inner)
    def _():
        z_send(2).start()

    for h in (0, 1):
        second(h, 0).start()
    to_other(OWN, 0).start()
    for rel in (XN, YN, DG):
        ap_recv(rel).wait_recv()
    az_copy(1).start()
    ao_copy(0).start()
    relay(0)
    take(1)
    pass_on(1)
    pass_on(2)
    az_copy(2).start()
    az_copy(3).start()
    sides(0)
    tabulate()
    for w in weights:
        w.wait()

    lane = lax.broadcasted_iota(jnp.int32, (rows, LANES), 1)
    steps = 2 * nz
    before, middle, after = {}, {}, {}

    def put(table, s, work, *args):
        table.setdefault(s, []).append(functools.partial(work, *args))

    end = nz - 1
    put(before, 1, relay, 1)
    put(middle, 0, corner, 0)
    put(middle, 1, pass_on, end)
    for k in range(1, nz):
        if k < end:
            put(middle, 2 * k - 1, take, k + 1)
            put(middle, 2 * k, relay, k + 1)
        else:
            put(middle, 2 * k, stage2, 1)
        put(middle, 2 * k - 1, sides, k)
        put(middle, 2 * k, corner, k)
    for s in range(1, 2 * end):
        put(after, s, merge, s - 1)
    for k in range(1, end - 1):
        put(after, 2 * k + 2, spread_along, k)
    put(before, 2 * end - 1, stage1, 1)
    put(middle, 2 * end, merge, 2 * end - 1)
    put(middle, 2 * end, stage1, end - 1)
    put(middle, 2 * end, spread_along, end - 1)
    put(middle, 2 * end + 1, merge, 2 * end)

    @pl.loop(0, steps)
    def _(s):
        for at, works in before.items():
            @pl.when(s == at)
            def _():
                for work in works:
                    work()

        k = s // 2
        side = s % 2
        at_z = jnp.where(k < 2, 2 * (z // 2) + (z + k) % 2, k + (z // 2) * (nz - 1 - 2 * k))
        for b in (0, 1):
            column = jnp.where(side == 0, columns[b], columns[2 + b])
            at = xbuf.at[1 - c, at_z * n_sp + column, :, body]
            n = k * n_sp + 2 * side + b
            rc(at, at, s_p, r_p.at[n], other).wait_recv()

        @pl.when(side == 0)
        def _():
            at = xbuf.at[1 - c, pl.ds(at_z * n_sp, n_sp), :, along]
            rc(at, at, s_ao, r_ao.at[k], other).wait_recv()

        i = couple(at_z, s)
        held = xbuf[:, i].reshape(4 * rows, width)
        row = y + side - 2 * y * side
        scale = jnp.concatenate(
            [
                jnp.sum(
                    jnp.where(
                        lane == (at_z * 2 + core) * n_sp + 2 * row + e,
                        turned_table[pl.ds(0, rows)], 0.0,
                    ),
                    axis=1,
                    keepdims=True,
                )
                for core in (0, 1)
                for e in (0, 1)
            ],
            axis=0,
        )
        gate = jnp.dot(held, wg[...], preferred_element_type=f32)
        up = jnp.dot(held, wu[...], preferred_element_type=f32)
        acts[...] = (jax.nn.silu(gate) * up * scale).astype(acts.dtype)

        for at, works in middle.items():
            @pl.when(s == at)
            def _():
                for work in works:
                    work()

        down = jnp.dot(acts[...], wd[...], preferred_element_type=f32)
        pbuf[:, i] = down.astype(pbuf.dtype).reshape(2, 2, rows, width)
        rc(pbuf.at[1 - c, i], dbuf.at[i], s_d, r_d.at[s], other).start()

        for at, works in after.items():
            @pl.when(s == at)
            def _():
                for work in works:
                    work()

    stage3(1)
    stage2(end - 1)
    merge(2 * end + 1)
    stage1(end)
    stage3(end - 1)
    spread_along(end)
    stage2(end)
    stage1(0)
    stage4(end - 1)
    stage3(end)
    stage2(0)
    along_sum()
    stage4(end)
    for h in (0, 1):
        total = hid[:, part(h)].astype(f32) + summed(h, 0)
        for n in (0, 1):
            rz_copy(h, n + 1).wait_recv()
            total = total + rz[n, :, part(h)].astype(f32)
        out_ref[:, part(h)] = total.astype(out_ref.dtype)
    total = hid[:, along].astype(f32) + pbuf[c, slot(0, OWN), :, along].astype(f32)
    for rel in (XN, YN, DG):
        bp_copy(rel).wait_recv()
        total = total + rbp[rel].astype(f32)
    out_ref[:, along] = total.astype(out_ref.dtype)

    for copy in halo_copies():
        copy.wait_send()
    swaps().wait_send()
    tables().wait_send()
    for h in (0, 1):
        rz_copy(h, 1).wait_send()
    z_send(1).wait_send()

    @pl.when(inner)
    def _():
        z_send(2).wait_send()
        for k in range(1, nz):
            forward(k).wait_send()
        for k in range(2, nz):
            for h in (0, 1):
                rz_copy(h, k).wait_send()

    @pl.when(outer)
    def _():
        for k in range(2, nz):
            for h in (0, 1):
                mate_copy(h, k).wait_send()

    def sent(at, ss):
        rc(at, at, ss, r_t, other).wait_send()

    every = nz * n_sp
    sent(named.at[pl.ds(0, n_sp - 1)], s_n)
    sent(xbuf.at[c, pl.ds(0, 2 * nz), :, part(0)], s_1)
    sent(xbuf.at[c, pl.ds(0, every), :, part(0)], s_2)
    sent(xbuf.at[c, pl.ds(0, every), :, body], s_p)
    sent(xbuf.at[c, pl.ds(0, n_sp - 1), :, along], s_ap)
    sent(xbuf.at[c, pl.ds(0, every - n_sp), :, along], s_az)
    sent(xbuf.at[c, pl.ds(0, every), :, along], s_ao)
    sent(pbuf.at[c], s_d)
    sent(pbuf.at[c, pl.ds(0, every), :, part(0)], s_r1)
    sent(pbuf.at[c, pl.ds(0, 2 * nz), :, part(0)], s_r2)
    sent(pbuf.at[c, pl.ds(0, every - n_sp), :, along], s_bz)
    sent(rbp.at[pl.ds(0, n_sp - 1)], s_bp)


def layer(gate_b, gate_c, values_in, conv_w, docs, resid, gain, ids, route, w_out, w_gate, w_up, w_down):
    rows, width = resid.shape
    seq, held = gate_b.shape
    n_tp = lax.axis_size("tp")
    n_sp = lax.axis_size("sp")
    nz = n_tp // 2
    quarter = width // 8
    share = (width - quarter) // 2
    bf = jnp.bfloat16
    f32 = jnp.float32
    dma = pltpu.SemaphoreType.DMA
    hbm = pl.BlockSpec(memory_space=pl.ANY)
    vmem = pl.BlockSpec(memory_space=pltpu.VMEM)
    operands = (gate_b, gate_c, values_in, conv_w, docs, resid, gain, ids, route)
    return pl.pallas_call(
        moe_kernel,
        out_shape=pltpu.VMEM((rows, width), bf),
        in_specs=[hbm] * 13,
        out_specs=vmem,
        scratch_shapes=[pltpu.VMEM(a.shape, a.dtype) for a in operands] + [
            pltpu.VMEM((rows, width), bf),
            pltpu.VMEM((rows, n_tp * held), bf),
            pltpu.VMEM((seq, held), bf),
            pltpu.VMEM((seq + 8, held), f32),
            pltpu.VMEM((seq + 8, held), f32),
            pltpu.VMEM((LANES, LANES), f32),
            pltpu.VMEM((16, held), bf),
            pltpu.VMEM((16, held), bf),
            pltpu.VMEM(docs.shape, docs.dtype),
            pltpu.VMEM(w_out.shape, bf),
            pltpu.VMEM((n_sp, 1, LANES), f32),
            pltpu.VMEM((n_sp, 1, LANES), f32),
            pltpu.VMEM((n_tp, n_sp, 1, LANES), f32),
            pltpu.VMEM((LANES, LANES), f32),
            pltpu.VMEM((2, n_sp * nz, rows, width), bf),
            pltpu.VMEM((2, n_sp * nz, rows, width), bf),
            pltpu.VMEM((n_sp * nz, rows, width), bf),
            pltpu.VMEM((2, 2, nz, rows, share), bf),
            pltpu.VMEM((2, nz, rows, share), bf),
            pltpu.VMEM((2, rows, 2 * share), bf),
            pltpu.VMEM((2, rows, 2 * share), bf),
            pltpu.VMEM((nz, n_sp, rows, quarter), bf),
            pltpu.VMEM((4, rows, quarter), bf),
            pltpu.VMEM((4 * rows, w_gate.shape[1]), bf),
            pltpu.VMEM(w_gate.shape, bf),
            pltpu.VMEM(w_up.shape, bf),
            pltpu.VMEM(w_down.shape, bf),
            dma((9,)), dma((4,)),
            dma, dma, dma((3,)), dma((3,)), dma, dma((4,)), dma, dma,
            dma((nz,)), dma((nz,)), dma((nz,)), dma, dma, dma((2, 4, nz)), dma, dma((n_sp * nz,)),
            dma, dma((2 * nz,)), dma, dma((2, 2, nz)), dma, dma((2, nz)),
            dma((2, 2)), dma((2, 2)), dma((nz, 2)), dma((2, 2)),
            dma, dma((nz,)), dma, dma((4,)), dma, dma((4,)), dma, dma((nz,)), dma, dma((nz,)),
        ],
        compiler_params=pltpu.CompilerParams(
            collective_id=0, has_side_effects=True, vmem_limit_bytes=64000000
        ),
    )(*operands, w_out, w_gate, w_up, w_down)


def passed_along(block, axis, distance):
    devices = range(lax.axis_size(axis))
    route = [(i - distance, i) for i in devices if i - distance in devices]
    return lax.ppermute(block, axis, route)


def local(
    gate_b,
    gate_c,
    values_in,
    conv_w,
    documents,
    w_out,
    resid,
    norm_gain,
    route_ids,
    route_weight,
    w_gate,
    w_up,
    w_down,
):
    seq_rows = gate_b.shape[0]
    local_rows = resid.shape[0]
    model_width = resid.shape[1]
    experts = lax.axis_size("sp") * w_gate.shape[0]
    capacity = 4 * local_rows // experts
    if (lax.axis_size("sp"), lax.axis_size("tp")) == (4, 8) and w_gate.shape[0] == 1 and capacity >= local_rows:
        return layer(
            gate_b, gate_c, values_in, conv_w, documents.reshape(-1, LANES), resid,
            norm_gain.reshape(-1, LANES), route_ids.T, route_weight.T,
            w_out, w_gate[0], w_up[0], w_down[0],
        )
    last_rows = jnp.stack([gate_c[seq_rows - 2 :], values_in[seq_rows - 2 :]])
    before, before_docs = passed_along((last_rows, documents[seq_rows - 2 :]), "sp", 1)
    products = jnp.concatenate(
        [
            before[0].astype(jnp.float32) * before[1].astype(jnp.float32),
            gate_c.astype(jnp.float32) * values_in.astype(jnp.float32),
        ],
        axis=0,
    )
    docs_all = jnp.concatenate([before_docs, documents], axis=0)
    kernel_taps = conv_w.astype(jnp.float32)
    near_mask = (docs_all[1:-1] == documents).astype(jnp.float32)[:, None]
    far_mask = (docs_all[:-2] == documents).astype(jnp.float32)[:, None]
    convolved = (
        kernel_taps[2] * products[2:]
        + kernel_taps[1] * products[1:-1] * near_mask
        + kernel_taps[0] * products[:-2] * far_mask
    )
    mixed_rows = (gate_b.astype(jnp.float32) * convolved).astype(jnp.bfloat16)
    token_rows = lax.all_to_all(mixed_rows, "tp", split_axis=0, concat_axis=1, tiled=True)
    projected = jnp.dot(token_rows, w_out, preferred_element_type=jnp.float32)
    hidden_state = (resid.astype(jnp.float32) + projected).astype(jnp.bfloat16)
    state_wide = hidden_state.astype(jnp.float32)
    normed = (
        state_wide
        * lax.rsqrt(jnp.mean(state_wide * state_wide, axis=-1, keepdims=True) + 1e-06)
        * norm_gain.astype(jnp.float32)
    ).astype(jnp.bfloat16)
    experts = lax.axis_size("sp") * w_gate.shape[0]
    capacity = 4 * local_rows // experts
    flat_ids = route_ids.reshape(-1)
    one_hot = (flat_ids[:, None] == jnp.arange(experts, dtype=jnp.int32)[None, :]).astype(jnp.int32)
    rank_in = jnp.sum((jnp.cumsum(one_hot, axis=0) - one_hot) * one_hot, axis=1)
    slot_index = flat_ids * capacity + rank_in
    placement = (
        slot_index[:, None] == jnp.arange(experts * capacity, dtype=jnp.int32)[None, :]
    ).astype(jnp.bfloat16)
    repeated = jnp.repeat(normed, 2, axis=0)
    dispatch = jnp.einsum(
        "js,jd->sd", placement, repeated, preferred_element_type=jnp.float32
    ).astype(jnp.bfloat16)
    dispatch = dispatch.reshape(experts, capacity, model_width)
    gathered_piece = lax.all_gather(
        lax.all_to_all(dispatch, "sp", split_axis=0, concat_axis=0, tiled=True),
        "tp",
        axis=0,
        tiled=True,
    )
    flat_rows = gathered_piece.reshape(-1, model_width)
    gate_part = jnp.dot(flat_rows, w_gate[0], preferred_element_type=jnp.float32)
    up_part = jnp.dot(flat_rows, w_up[0], preferred_element_type=jnp.float32)
    activated = (jax.nn.silu(gate_part) * up_part).astype(jnp.bfloat16)
    partial_value = jnp.dot(activated, w_down[0], preferred_element_type=jnp.float32)
    partial_value = partial_value.reshape(
        gathered_piece.shape[0], gathered_piece.shape[1], model_width
    )
    summed = lax.psum_scatter(
        partial_value.astype(jnp.bfloat16), "tp", scatter_dimension=0, tiled=True
    )
    returned = lax.all_to_all(summed, "sp", split_axis=0, concat_axis=0, tiled=True)
    picked = jnp.take(
        returned.reshape(experts * capacity, model_width), slot_index, axis=0
    ).reshape(local_rows, 2, model_width)
    combined = jnp.sum(route_weight[:, :, None] * picked.astype(jnp.float32), axis=1)
    return (hidden_state.astype(jnp.float32) + combined).astype(jnp.bfloat16)


def solution(mesh):
    return jax.shard_map(
        local,
        mesh=mesh,
        in_specs=(
            P("sp", "tp"),
            P("sp", "tp"),
            P("sp", "tp"),
            P(None, "tp"),
            P("sp"),
            P(),
            P(("sp", "tp"), None),
            P(),
            P(("sp", "tp"), None),
            P(("sp", "tp"), None),
            P("sp", None, "tp"),
            P("sp", None, "tp"),
            P("sp", "tp", None),
        ),
        out_specs=P(("sp", "tp"), None),
        check_vma=False,
    )
```

```python
import functools

import jax
import jax.numpy as jnp
from jax import lax
from jax.experimental import pallas as pl
from jax.experimental.pallas import tpu as pltpu
from jax.sharding import PartitionSpec as P

MESH = pl.DeviceIdType.MESH
LANES = 128


def moe_kernel(
    gb_hbm, gc_hbm, vals_hbm, taps_hbm, docs_hbm, resid_hbm, gain_hbm, ids_hbm, route_hbm,
    wo_hbm, wg_hbm, wu_hbm, wd_hbm, out_ref,
    gb, gc, vals, taps, docs, resid, gain, ids, route,
    hid, tok, mixed, pad, dpad, mat, hc, hv, hd, wo, named, shares, table, turned_table,
    xbuf, pbuf, dbuf, r1, r2, rm, rz, rbz, rbp, acts, wg, wu, wd,
    in_sem, w_sem,
    s_a, r_a, s_h, r_h3, s_n, r_n, s_t, r_t,
    s_z, s_f, r_z, s_1, s_2, r_h, s_p, r_p,
    s_d, r_d, s_r1, r_r1, s_r2, r_r2, s_m, r_m, s_rz, r_rz,
    s_bz, r_bz, s_bp, r_bp, s_ap, r_ap, s_az, r_az, s_ao, r_ao,
):
    f32 = jnp.float32
    n_sp, n_tp = lax.axis_size("sp"), lax.axis_size("tp")
    nz = n_tp // 2
    width = out_ref.shape[1]
    half = width // 2
    rows = out_ref.shape[0]
    seq = gb.shape[0]
    halo = hc.shape[0]
    sp, tp = lax.axis_index("sp"), lax.axis_index("tp")
    y, x = sp // 2, sp % 2
    z, c = tp // 2, tp % 2
    xn, yn, dg = y * 2 + 1 - x, (1 - y) * 2 + x, (1 - y) * 2 + 1 - x
    columns = (sp, xn, yn, dg)
    OWN, XN, YN, DG = range(4)
    other = (sp, z * 2 + 1 - c)
    following, previous = (lax.rem(sp + 1, n_sp), tp), (lax.rem(sp + n_sp - 1, n_sp), tp)
    to_x, to_y = (xn, tp), (yn, tp)
    inner = z % 2 != z // 2
    outer = z % 2 == z // 2

    def zz(k):
        if k < 2:
            return 2 * (z // 2) + (z + k) % 2
        return k + (z // 2) * (nz - 1 - 2 * k)

    def slot(k, rel):
        return zz(k) * n_sp + columns[rel]

    def cols(h):
        return pl.ds(h * half, half)

    quarter = rbz.shape[3]
    share = (width - quarter) // 2

    def part(h):
        return pl.ds(h * share, share)

    body = pl.ds(0, 2 * share)
    along = pl.ds(2 * share, quarter)

    def rc(src, dst, ss, rs, dev):
        return pltpu.make_async_remote_copy(
            src_ref=src, dst_ref=dst, send_sem=ss, recv_sem=rs,
            device_id=dev, device_id_type=MESH,
        )


    def halo_copies():
        pairs = (
            (gc.at[pl.ds(seq - halo, halo)], hc),
            (vals.at[pl.ds(seq - halo, halo)], hv),
            (docs, hd),
        )
        return [rc(a, b, s_h.at[n], r_h3.at[n], following) for n, (a, b) in enumerate(pairs)]

    def channels(j):
        return pl.ds(pl.multiple_of(j * gb.shape[1], gb.shape[1]), gb.shape[1])

    def token_rows(j):
        return mixed.at[pl.ds(pl.multiple_of(j * rows, rows), rows)]

    def swap(d):
        j = lax.rem(tp + d, n_tp)
        return rc(token_rows(j), tok.at[:, channels(tp)], s_a, r_a, (sp, j))

    def swaps():
        at = tok.at[:, pl.ds(0, (n_tp - 1) * gb.shape[1])]
        return rc(at, at, s_a, r_a, other)

    def swap_first():
        return rc(token_rows(0), tok.at[:, channels(tp)], s_a, r_a, (sp, 0))


    def name_copy(rel):
        return rc(named.at[columns[rel]], shares.at[sp], s_n, r_n.at[rel], (columns[rel], tp))

    def table_copy(d):
        return rc(shares, table.at[tp], s_t, r_t, (sp, lax.rem(tp + d, n_tp)))

    def tables():
        at = table.at[pl.ds(0, n_tp - 1)]
        return rc(at, at, s_t, r_t, other)

    def name():
        named[...] = jnp.zeros_like(named)
        for e in range(n_sp):
            named[e, :, pl.ds(0, rows)] = jnp.where(ids[0:1] == e, route[0:1], 0.0) + jnp.where(
                ids[1:2] == e, route[1:2], 0.0
            )
        for rel in (XN, YN, DG):
            name_copy(rel).start()
        shares[sp] = named[sp]

    def tabulate():
        tables().wait_recv()
        mat[...] = jnp.zeros_like(mat)
        for j in range(n_tp):
            for e in range(n_sp):
                mat[pl.ds(j * n_sp + e, 1)] = table[j, e]
        turned_table[...] = mat[...].T

    def convolve(first, count):
        own = pl.ds(first, count)
        now = dpad[pl.ds(first + 8, count)]
        near = (dpad[pl.ds(first + 7, count)] == now).astype(f32)
        far = (dpad[pl.ds(first + 6, count)] == now).astype(f32)
        tap = taps[...].astype(f32)
        convolved = (
            tap[2:3] * pad[pl.ds(first + 8, count)]
            + tap[1:2] * pad[pl.ds(first + 7, count)] * near
            + tap[0:1] * pad[pl.ds(first + 6, count)] * far
        )
        mixed[own] = (gb[own].astype(f32) * convolved).astype(mixed.dtype)

    def mix():
        doc_rows = docs.shape[0]
        mat[...] = jnp.zeros_like(mat)
        mat[pl.ds(0, doc_rows)] = docs[...].astype(f32)
        turned = mat[...].T
        for n in range(doc_rows):
            dpad[pl.ds(8 + n * LANES, LANES)] = jnp.broadcast_to(
                turned[:, n : n + 1], (LANES, dpad.shape[1])
            )
        pad[pl.ds(8, seq)] = gc[...].astype(f32) * vals[...].astype(f32)
        pad[pl.ds(0, 8)] = jnp.zeros((8, pad.shape[1]), f32)
        dpad[pl.ds(0, 8)] = jnp.full((8, dpad.shape[1]), -1.0, f32)
        convolve(0, seq)
        for d in range(1, n_tp):
            @pl.when(lax.rem(tp + d, n_tp) != 0)
            def _():
                swap(d).start()

        mine = z * n_sp + sp

        for copy in halo_copies():
            copy.wait_recv()
        pad[pl.ds(0, 8)] = (hc[...].astype(f32) * hv[...].astype(f32))[halo - 8 :]
        last = hd[pl.ds(doc_rows - 1, 1)].astype(f32)
        last = jnp.where(sp == 0, -1.0, last)
        for n in (1, 2):
            dpad[pl.ds(8 - n, 1)] = jnp.broadcast_to(
                last[:, LANES - n : LANES - n + 1], (1, dpad.shape[1])
            )
        convolve(0, 16)

        @pl.when(tp != 0)
        def _():
            swap_first().start()

        for rel in (XN, YN, DG):
            name_copy(rel).wait_recv()
        table[tp] = shares[...]
        for d in range(1, n_tp):
            table_copy(d).start()

        tok[:, channels(tp)] = mixed[pl.ds(pl.multiple_of(tp * rows, rows), rows)]
        in_copies[5].wait()
        in_copies[6].wait()
        wo_copy.wait()
        swaps().wait_recv()
        projected = jnp.dot(tok[...], wo[...], preferred_element_type=f32)
        hidden = (resid[...].astype(f32) + projected).astype(hid.dtype)
        hid[...] = hidden
        state = hidden.astype(f32)
        scale = lax.rsqrt(jnp.mean(state * state, axis=-1, keepdims=True) + 1e-06)
        for n in range(width // LANES):
            at = slice(n * LANES, (n + 1) * LANES)
            xbuf[c, mine, :, pl.ds(n * LANES, LANES)] = (
                state[:, at] * scale * gain[n : n + 1].astype(f32)
            ).astype(xbuf.dtype)


    def z_send(k):
        at = xbuf.at[c, z * n_sp + sp, :, body]
        return rc(at, at, s_z.at[k], r_z.at[z], (sp, zz(k) * 2 + c))

    def z_recv(k):
        at = xbuf.at[c, slot(k, OWN), :, body]
        return rc(at, at, s_z.at[k], r_z.at[zz(k)], (sp, zz(k) * 2 + c))

    def forward(k):
        at = xbuf.at[c, slot(k, OWN), :, body]
        return rc(at, at, s_f.at[k], r_z.at[zz(k)], (sp, zz(2 if k == 1 else 1) * 2 + c))

    def pass_on(k):
        @pl.when(inner)
        def _():
            if k > 1:
                z_recv(k).wait_recv()
            forward(k).start()

    def piece(h, rel, k, ss, there, dev):
        at = xbuf.at[c, slot(k, rel), :, part(h)]
        return rc(at, at, ss, r_h.at[h, there, k], dev)

    def first(h, k):
        return piece(h, OWN, k, s_1, YN if h == 0 else XN, to_y if h == 0 else to_x)

    def second(h, k):
        return piece(h, OWN, k, s_2, XN if h == 0 else YN, to_x if h == 0 else to_y)

    def third(h, k):
        return piece(h, YN if h == 0 else XN, k, s_2, DG, to_x if h == 0 else to_y)

    def arrived(h, rel, k):
        piece(h, rel, k, s_1, rel, other).wait_recv()

    def to_other(rel, k):
        at = xbuf.at[c, slot(k, rel), :, body]
        return rc(at, at, s_p, r_p.at[k * n_sp + rel], other)


    def ap_copy(rel):
        at = xbuf.at[c, z * n_sp + sp, :, along]
        return rc(at, at, s_ap, r_ap.at[rel], (columns[rel], tp))

    def ap_recv(rel):
        at = xbuf.at[c, slot(0, rel), :, along]
        return rc(at, at, s_ap, r_ap.at[rel], (columns[rel], tp))

    def az_copy(k):
        at = xbuf.at[c, pl.ds(z * n_sp, n_sp), :, along]
        return rc(at, at, s_az, r_az.at[z], (sp, zz(k) * 2 + c))

    def az_recv(k):
        at = xbuf.at[c, group(k), :, along]
        return rc(at, at, s_az, r_az.at[zz(k)], (sp, zz(k) * 2 + c))

    def ao_copy(k):
        at = xbuf.at[c, group(k), :, along]
        return rc(at, at, s_ao, r_ao.at[k], other)

    def spread(k):
        for h in (1, 0):
            first(h, k).start()
        for h in (0, 1):
            second(h, k).start()
        to_other(OWN, k).start()

    def take(k):
        if k == 1:
            z_recv(k).wait_recv()
        else:
            @pl.when(outer)
            def _():
                z_recv(k).wait_recv()
        spread(k)

    def relay(k):
        arrived(0, YN, k)
        third(0, k).start()
        arrived(1, XN, k)
        third(1, k).start()

    def sides(k):
        if k > 0:
            az_recv(k).wait_recv()
            ao_copy(k).start()
        arrived(0, XN, k)
        to_other(XN, k).start()
        arrived(1, YN, k)
        to_other(YN, k).start()

    def corner(k):
        arrived(0, DG, k)
        arrived(1, DG, k)
        to_other(DG, k).start()


    def group(k):
        return pl.ds(zz(k) * n_sp, n_sp)

    def couple(at_z, s):
        row = y + s % 2 - 2 * y * (s % 2)
        return pl.ds(at_z * n_sp + 2 * row, 2)

    def d_copy(s):
        i = couple(zz(s // 2), s)
        return rc(pbuf.at[1 - c, i], dbuf.at[i], s_d, r_d.at[s], other)

    def merge(s):
        d_copy(s).wait_recv()
        i = couple(zz(s // 2), s)
        pbuf[c, i] = (pbuf[c, i].astype(f32) + dbuf[i].astype(f32)).astype(pbuf.dtype)

    def spread_along(k):
        bz_copy(k).start()

    def r1_copy(h, o, k):
        rel = DG if o else (XN if h == 0 else YN)
        at = pbuf.at[c, slot(k, rel), :, part(h)]
        return rc(at, r1.at[h, o, k], s_r1, r_r1.at[h, o, k], to_x if h == 0 else to_y)

    def r2_copy(h, k):
        at = pbuf.at[c, slot(k, YN if h == 0 else XN), :, part(h)]
        return rc(at, r2.at[h, k], s_r2, r_r2.at[h, k], to_y if h == 0 else to_x)

    def mate_copy(h, k):
        at = pbuf.at[c, slot(k, OWN), :, part(h)]
        return rc(at, rm.at[k - 2, :, part(h)], s_m.at[k - 2, h], r_m.at[k - 2, h], (sp, zz(1) * 2 + c))

    def rz_copy(h, k):
        n = min(k - 1, 1)
        at = pbuf.at[c, slot(k, OWN), :, part(h)]
        return rc(at, rz.at[n, :, part(h)], s_rz.at[k, h], r_rz.at[n, h], (sp, zz(k) * 2 + c))

    def bz_copy(k):
        return rc(
            pbuf.at[c, group(k), :, along], rbz.at[z], s_bz, r_bz.at[z], (sp, zz(k) * 2 + c)
        )

    def bz_recv(k):
        return rc(
            pbuf.at[c, group(k), :, along], rbz.at[zz(k)], s_bz, r_bz.at[zz(k)],
            (sp, zz(k) * 2 + c),
        )

    def bp_copy(rel):
        return rc(
            pbuf.at[c, slot(0, rel), :, along], rbp.at[rel], s_bp, r_bp.at[rel],
            (columns[rel], tp),
        )

    def along_sum():
        total = pbuf[c, group(0), :, along].astype(f32)
        for k in range(1, nz):
            bz_recv(k).wait_recv()
            total = total + rbz[zz(k)].astype(f32)
        pbuf[c, group(0), :, along] = total.astype(pbuf.dtype)
        for rel in (DG, XN, YN):
            bp_copy(rel).start()

    def stage1(k, parts=(1, 0)):
        for o in parts:
            for h in (0, 1):
                r1_copy(h, o, k).start()

    def stage2(k):
        for h in (0, 1):
            r1_copy(h, 1, k).wait_recv()
            i = slot(k, YN if h == 0 else XN)
            pbuf[c, i, :, part(h)] = (
                pbuf[c, i, :, part(h)].astype(f32) + r1[h, 1, k].astype(f32)
            ).astype(pbuf.dtype)
            r2_copy(h, k).start()

    def summed(h, k):
        r1_copy(h, 0, k).wait_recv()
        r2_copy(h, k).wait_recv()
        return (
            pbuf[c, slot(k, OWN), :, part(h)].astype(f32)
            + r1[h, 0, k].astype(f32)
            + r2[h, k].astype(f32)
        )

    def stage3(k):
        for h in (0, 1):
            pbuf[c, slot(k, OWN), :, part(h)] = summed(h, k).astype(pbuf.dtype)
            if k == 1:
                rz_copy(h, k).start()
            else:
                @pl.when(outer)
                def _():
                    mate_copy(h, k).start()

    def stage4(k):
        @pl.when(inner)
        def _():
            at = slot(k, OWN)
            for h in (0, 1):
                mate_copy(h, k).wait_recv()
                pbuf[c, at, :, part(h)] = (
                    pbuf[c, at, :, part(h)].astype(f32) + rm[k - 2, :, part(h)].astype(f32)
                ).astype(pbuf.dtype)
                rz_copy(h, k).start()

    barrier = pltpu.get_barrier_semaphore()
    peers = [to_x, to_y, (dg, tp), following, previous] + [(sp, lax.rem(tp + d, n_tp)) for d in range(1, n_tp)]
    for peer in peers:
        pl.semaphore_signal(barrier, inc=1, device_id=peer, device_id_type=MESH)
    in_copies = [
        pltpu.make_async_copy(a, b, in_sem.at[n])
        for n, (a, b) in enumerate((
            (gc_hbm, gc), (vals_hbm, vals), (docs_hbm, docs), (taps_hbm, taps), (gb_hbm, gb),
            (resid_hbm, resid), (gain_hbm, gain), (ids_hbm, ids), (route_hbm, route),
        ))
    ]
    weights = [
        pltpu.make_async_copy(a, b, w_sem.at[n])
        for n, (a, b) in enumerate(((wg_hbm, wg), (wu_hbm, wu), (wd_hbm, wd)))
    ]
    wo_copy = pltpu.make_async_copy(wo_hbm, wo, w_sem.at[3])
    for copy in in_copies:
        copy.start()
    wo_copy.start()
    for w in weights:
        w.start()
    for n in (0, 1, 2):
        in_copies[n].wait()
    pl.semaphore_wait(barrier, len(peers))
    for copy in halo_copies():
        copy.start()
    for n in (3, 4, 7, 8):
        in_copies[n].wait()
    name()
    mix()
    for rel in (DG, XN, YN):
        ap_copy(rel).start()
    for h in (1, 0):
        first(h, 0).start()
    z_send(1).start()

    @pl.when(inner)
    def _():
        z_send(2).start()

    for h in (0, 1):
        second(h, 0).start()
    to_other(OWN, 0).start()
    for rel in (XN, YN, DG):
        ap_recv(rel).wait_recv()
    az_copy(1).start()
    ao_copy(0).start()
    relay(0)
    take(1)
    pass_on(1)
    pass_on(2)
    az_copy(2).start()
    az_copy(3).start()
    sides(0)
    tabulate()
    for w in weights:
        w.wait()

    lane = lax.broadcasted_iota(jnp.int32, (rows, LANES), 1)
    steps = 2 * nz
    before, middle, after = {}, {}, {}

    def put(table, s, work, *args):
        table.setdefault(s, []).append(functools.partial(work, *args))

    end = nz - 1
    put(before, 1, relay, 1)
    put(middle, 0, corner, 0)
    put(before, 2, pass_on, end)
    for k in range(1, nz):
        if k < end:
            put(middle, 2 * k - 1, take, k + 1)
            put(middle, 2 * k, relay, k + 1)
        else:
            put(middle, 2 * k, stage2, 1)
        put(middle, 2 * k - 1, sides, k)
        put(middle, 2 * k, corner, k)
    for s in range(1, 2 * end):
        put(after, s, merge, s - 1)
    for k in range(1, end - 1):
        put(after, 2 * k + 2, spread_along, k)
    put(before, 2 * end - 1, stage1, 1)
    put(middle, 2 * end, merge, 2 * end - 1)
    put(middle, 2 * end, stage1, end - 1)
    put(middle, 2 * end, spread_along, end - 1)
    put(middle, 2 * end + 1, merge, 2 * end)

    @pl.loop(0, steps)
    def _(s):
        for at, works in before.items():
            @pl.when(s == at)
            def _():
                for work in works:
                    work()

        k = s // 2
        side = s % 2
        at_z = jnp.where(k < 2, 2 * (z // 2) + (z + k) % 2, k + (z // 2) * (nz - 1 - 2 * k))
        for b in (0, 1):
            column = jnp.where(side == 0, columns[b], columns[2 + b])
            at = xbuf.at[1 - c, at_z * n_sp + column, :, body]
            n = k * n_sp + 2 * side + b
            rc(at, at, s_p, r_p.at[n], other).wait_recv()

        @pl.when(side == 0)
        def _():
            at = xbuf.at[1 - c, pl.ds(at_z * n_sp, n_sp), :, along]
            rc(at, at, s_ao, r_ao.at[k], other).wait_recv()

        i = couple(at_z, s)
        held = xbuf[:, i].reshape(4 * rows, width)
        row = y + side - 2 * y * side
        scale = jnp.concatenate(
            [
                jnp.sum(
                    jnp.where(
                        lane == (at_z * 2 + core) * n_sp + 2 * row + e,
                        turned_table[pl.ds(0, rows)], 0.0,
                    ),
                    axis=1,
                    keepdims=True,
                )
                for core in (0, 1)
                for e in (0, 1)
            ],
            axis=0,
        )
        gate = jnp.dot(held, wg[...], preferred_element_type=f32)
        up = jnp.dot(held, wu[...], preferred_element_type=f32)
        acts[...] = (jax.nn.silu(gate) * up * scale).astype(acts.dtype)

        for at, works in middle.items():
            @pl.when(s == at)
            def _():
                for work in works:
                    work()

        down = jnp.dot(acts[...], wd[...], preferred_element_type=f32)
        pbuf[:, i] = down.astype(pbuf.dtype).reshape(2, 2, rows, width)
        rc(pbuf.at[1 - c, i], dbuf.at[i], s_d, r_d.at[s], other).start()

        for at, works in after.items():
            @pl.when(s == at)
            def _():
                for work in works:
                    work()

    stage3(1)
    stage2(end - 1)
    merge(2 * end + 1)
    stage1(end)
    stage3(end - 1)
    spread_along(end)
    stage2(end)
    stage1(0)
    stage4(end - 1)
    stage3(end)
    stage2(0)
    along_sum()
    stage4(end)
    for h in (0, 1):
        total = hid[:, part(h)].astype(f32) + summed(h, 0)
        for n in (0, 1):
            rz_copy(h, n + 1).wait_recv()
            total = total + rz[n, :, part(h)].astype(f32)
        out_ref[:, part(h)] = total.astype(out_ref.dtype)
    total = hid[:, along].astype(f32) + pbuf[c, slot(0, OWN), :, along].astype(f32)
    for rel in (XN, YN, DG):
        bp_copy(rel).wait_recv()
        total = total + rbp[rel].astype(f32)
    out_ref[:, along] = total.astype(out_ref.dtype)

    for copy in halo_copies():
        copy.wait_send()
    swaps().wait_send()
    tables().wait_send()
    for h in (0, 1):
        rz_copy(h, 1).wait_send()
    z_send(1).wait_send()

    @pl.when(inner)
    def _():
        z_send(2).wait_send()
        for k in range(1, nz):
            forward(k).wait_send()
        for k in range(2, nz):
            for h in (0, 1):
                rz_copy(h, k).wait_send()

    @pl.when(outer)
    def _():
        for k in range(2, nz):
            for h in (0, 1):
                mate_copy(h, k).wait_send()

    def sent(at, ss):
        rc(at, at, ss, r_t, other).wait_send()

    every = nz * n_sp
    sent(named.at[pl.ds(0, n_sp - 1)], s_n)
    sent(xbuf.at[c, pl.ds(0, 2 * nz), :, part(0)], s_1)
    sent(xbuf.at[c, pl.ds(0, every), :, part(0)], s_2)
    sent(xbuf.at[c, pl.ds(0, every), :, body], s_p)
    sent(xbuf.at[c, pl.ds(0, n_sp - 1), :, along], s_ap)
    sent(xbuf.at[c, pl.ds(0, every - n_sp), :, along], s_az)
    sent(xbuf.at[c, pl.ds(0, every), :, along], s_ao)
    sent(pbuf.at[c], s_d)
    sent(pbuf.at[c, pl.ds(0, every), :, part(0)], s_r1)
    sent(pbuf.at[c, pl.ds(0, 2 * nz), :, part(0)], s_r2)
    sent(pbuf.at[c, pl.ds(0, every - n_sp), :, along], s_bz)
    sent(rbp.at[pl.ds(0, n_sp - 1)], s_bp)


def layer(gate_b, gate_c, values_in, conv_w, docs, resid, gain, ids, route, w_out, w_gate, w_up, w_down):
    rows, width = resid.shape
    seq, held = gate_b.shape
    n_tp = lax.axis_size("tp")
    n_sp = lax.axis_size("sp")
    nz = n_tp // 2
    quarter = width // 8
    share = (width - quarter) // 2
    bf = jnp.bfloat16
    f32 = jnp.float32
    dma = pltpu.SemaphoreType.DMA
    hbm = pl.BlockSpec(memory_space=pl.ANY)
    vmem = pl.BlockSpec(memory_space=pltpu.VMEM)
    operands = (gate_b, gate_c, values_in, conv_w, docs, resid, gain, ids, route)
    return pl.pallas_call(
        moe_kernel,
        out_shape=pltpu.VMEM((rows, width), bf),
        in_specs=[hbm] * 13,
        out_specs=vmem,
        scratch_shapes=[pltpu.VMEM(a.shape, a.dtype) for a in operands] + [
            pltpu.VMEM((rows, width), bf),
            pltpu.VMEM((rows, n_tp * held), bf),
            pltpu.VMEM((seq, held), bf),
            pltpu.VMEM((seq + 8, held), f32),
            pltpu.VMEM((seq + 8, held), f32),
            pltpu.VMEM((LANES, LANES), f32),
            pltpu.VMEM((16, held), bf),
            pltpu.VMEM((16, held), bf),
            pltpu.VMEM(docs.shape, docs.dtype),
            pltpu.VMEM(w_out.shape, bf),
            pltpu.VMEM((n_sp, 1, LANES), f32),
            pltpu.VMEM((n_sp, 1, LANES), f32),
            pltpu.VMEM((n_tp, n_sp, 1, LANES), f32),
            pltpu.VMEM((LANES, LANES), f32),
            pltpu.VMEM((2, n_sp * nz, rows, width), bf),
            pltpu.VMEM((2, n_sp * nz, rows, width), bf),
            pltpu.VMEM((n_sp * nz, rows, width), bf),
            pltpu.VMEM((2, 2, nz, rows, share), bf),
            pltpu.VMEM((2, nz, rows, share), bf),
            pltpu.VMEM((2, rows, 2 * share), bf),
            pltpu.VMEM((2, rows, 2 * share), bf),
            pltpu.VMEM((nz, n_sp, rows, quarter), bf),
            pltpu.VMEM((4, rows, quarter), bf),
            pltpu.VMEM((4 * rows, w_gate.shape[1]), bf),
            pltpu.VMEM(w_gate.shape, bf),
            pltpu.VMEM(w_up.shape, bf),
            pltpu.VMEM(w_down.shape, bf),
            dma((9,)), dma((4,)),
            dma, dma, dma((3,)), dma((3,)), dma, dma((4,)), dma, dma,
            dma((nz,)), dma((nz,)), dma((nz,)), dma, dma, dma((2, 4, nz)), dma, dma((n_sp * nz,)),
            dma, dma((2 * nz,)), dma, dma((2, 2, nz)), dma, dma((2, nz)),
            dma((2, 2)), dma((2, 2)), dma((nz, 2)), dma((2, 2)),
            dma, dma((nz,)), dma, dma((4,)), dma, dma((4,)), dma, dma((nz,)), dma, dma((nz,)),
        ],
        compiler_params=pltpu.CompilerParams(
            collective_id=0, has_side_effects=True, vmem_limit_bytes=64000000
        ),
    )(*operands, w_out, w_gate, w_up, w_down)


def passed_along(block, axis, distance):
    devices = range(lax.axis_size(axis))
    route = [(i - distance, i) for i in devices if i - distance in devices]
    return lax.ppermute(block, axis, route)


def local(
    gate_b,
    gate_c,
    values_in,
    conv_w,
    documents,
    w_out,
    resid,
    norm_gain,
    route_ids,
    route_weight,
    w_gate,
    w_up,
    w_down,
):
    seq_rows = gate_b.shape[0]
    local_rows = resid.shape[0]
    model_width = resid.shape[1]
    experts = lax.axis_size("sp") * w_gate.shape[0]
    capacity = 4 * local_rows // experts
    if (lax.axis_size("sp"), lax.axis_size("tp")) == (4, 8) and w_gate.shape[0] == 1 and capacity >= local_rows:
        return layer(
            gate_b, gate_c, values_in, conv_w, documents.reshape(-1, LANES), resid,
            norm_gain.reshape(-1, LANES), route_ids.T, route_weight.T,
            w_out, w_gate[0], w_up[0], w_down[0],
        )
    last_rows = jnp.stack([gate_c[seq_rows - 2 :], values_in[seq_rows - 2 :]])
    before, before_docs = passed_along((last_rows, documents[seq_rows - 2 :]), "sp", 1)
    products = jnp.concatenate(
        [
            before[0].astype(jnp.float32) * before[1].astype(jnp.float32),
            gate_c.astype(jnp.float32) * values_in.astype(jnp.float32),
        ],
        axis=0,
    )
    docs_all = jnp.concatenate([before_docs, documents], axis=0)
    kernel_taps = conv_w.astype(jnp.float32)
    near_mask = (docs_all[1:-1] == documents).astype(jnp.float32)[:, None]
    far_mask = (docs_all[:-2] == documents).astype(jnp.float32)[:, None]
    convolved = (
        kernel_taps[2] * products[2:]
        + kernel_taps[1] * products[1:-1] * near_mask
        + kernel_taps[0] * products[:-2] * far_mask
    )
    mixed_rows = (gate_b.astype(jnp.float32) * convolved).astype(jnp.bfloat16)
    token_rows = lax.all_to_all(mixed_rows, "tp", split_axis=0, concat_axis=1, tiled=True)
    projected = jnp.dot(token_rows, w_out, preferred_element_type=jnp.float32)
    hidden_state = (resid.astype(jnp.float32) + projected).astype(jnp.bfloat16)
    state_wide = hidden_state.astype(jnp.float32)
    normed = (
        state_wide
        * lax.rsqrt(jnp.mean(state_wide * state_wide, axis=-1, keepdims=True) + 1e-06)
        * norm_gain.astype(jnp.float32)
    ).astype(jnp.bfloat16)
    experts = lax.axis_size("sp") * w_gate.shape[0]
    capacity = 4 * local_rows // experts
    flat_ids = route_ids.reshape(-1)
    one_hot = (flat_ids[:, None] == jnp.arange(experts, dtype=jnp.int32)[None, :]).astype(jnp.int32)
    rank_in = jnp.sum((jnp.cumsum(one_hot, axis=0) - one_hot) * one_hot, axis=1)
    slot_index = flat_ids * capacity + rank_in
    placement = (
        slot_index[:, None] == jnp.arange(experts * capacity, dtype=jnp.int32)[None, :]
    ).astype(jnp.bfloat16)
    repeated = jnp.repeat(normed, 2, axis=0)
    dispatch = jnp.einsum(
        "js,jd->sd", placement, repeated, preferred_element_type=jnp.float32
    ).astype(jnp.bfloat16)
    dispatch = dispatch.reshape(experts, capacity, model_width)
    gathered_piece = lax.all_gather(
        lax.all_to_all(dispatch, "sp", split_axis=0, concat_axis=0, tiled=True),
        "tp",
        axis=0,
        tiled=True,
    )
    flat_rows = gathered_piece.reshape(-1, model_width)
    gate_part = jnp.dot(flat_rows, w_gate[0], preferred_element_type=jnp.float32)
    up_part = jnp.dot(flat_rows, w_up[0], preferred_element_type=jnp.float32)
    activated = (jax.nn.silu(gate_part) * up_part).astype(jnp.bfloat16)
    partial_value = jnp.dot(activated, w_down[0], preferred_element_type=jnp.float32)
    partial_value = partial_value.reshape(
        gathered_piece.shape[0], gathered_piece.shape[1], model_width
    )
    summed = lax.psum_scatter(
        partial_value.astype(jnp.bfloat16), "tp", scatter_dimension=0, tiled=True
    )
    returned = lax.all_to_all(summed, "sp", split_axis=0, concat_axis=0, tiled=True)
    picked = jnp.take(
        returned.reshape(experts * capacity, model_width), slot_index, axis=0
    ).reshape(local_rows, 2, model_width)
    combined = jnp.sum(route_weight[:, :, None] * picked.astype(jnp.float32), axis=1)
    return (hidden_state.astype(jnp.float32) + combined).astype(jnp.bfloat16)


def solution(mesh):
    return jax.shard_map(
        local,
        mesh=mesh,
        in_specs=(
            P("sp", "tp"),
            P("sp", "tp"),
            P("sp", "tp"),
            P(None, "tp"),
            P("sp"),
            P(),
            P(("sp", "tp"), None),
            P(),
            P(("sp", "tp"), None),
            P(("sp", "tp"), None),
            P("sp", None, "tp"),
            P("sp", None, "tp"),
            P("sp", "tp", None),
        ),
        out_specs=P(("sp", "tp"), None),
        check_vma=False,
    )
```
